32 devices in a mesh: fs: 8 (over z, y), tp: 4 (over x, core).
Axes of the slice: x: 2, y: 2, z: 4, core: 2. Of those that a mesh axis runs over, the one named last changes fastest.
Arguments:
- tokens: bfloat16 [8192, 2048], P(('fs', 'tp')), may hold values from -6 to 6
- expert_group: int32 [8192], P(('fs', 'tp')), may hold values from 0 to 1, as said below
- expert_fine: int32 [8192, 2], P(('fs', 'tp')), may hold values from 0 to 3, as said below
- route_weight: float32 [8192, 2], P(('fs', 'tp')), may hold values from 0.2 to 0.9
- norm_gain: float32 [2048], P('fs'), may hold values from 0.1 to 1.9
- gate_master: float32 [8, 2048, 512], P(None, 'fs', 'tp'), may hold values from -0.125 to 0.125
- up_master: float32 [8, 2048, 512], P(None, 'fs', 'tp'), may hold values from -0.125 to 0.125
- down_master: float32 [8, 2048, 512], P(None, 'fs', 'tp'), may hold values from -0.25 to 0.25
Outputs:
- mixed: bfloat16 [8192, 2048], P(('fs', 'tp'))
- gate_ready: bfloat16 [8, 2048, 512], P('fs')
- up_ready: bfloat16 [8, 2048, 512], P('fs')
- down_ready: bfloat16 [8, 2048, 512], P('fs')
The draws below stay inside these ranges and needn't reach their ends.
Inputs may be any that keep to these rules, and one draw needn't show every extreme that they name: `expert_group`: in the rows of one device every group is chosen by the same number of rows. `expert_fine`: the two entries of a row differ. Counting an expert as its group and entry, the rows of one device name one expert at most 128 times, and in every group one expert is named exactly 128 times by the rows of every device.
All inputs are finite; a program needn't handle non-finite values.
Results may differ from the reference program's by a relative error of at most 0.0086.
Values may be sent and summed in bfloat16 or wider, within the bound.
A program may use at most 128 MiB of HBM per device.

```python
import jax
import jax.numpy as jnp
from jax import lax

D = 2048
F = 512
FINE = 4
TOP = 2
TOK_DEV = 256
EXPERTS = 8
GROUPS = 2
CAP = 128
TOKENS = 8192
DEVICES = 32


def route_tables(key):
    base = jax.random.fold_in(key, 7)
    blocks = TOKENS // TOK_DEV
    per_group = TOK_DEV // GROUPS
    pattern = jnp.array([16, 8, 5, 3], jnp.int32)
    hot_key = jax.random.fold_in(base, 1)
    perm_key = jax.random.fold_in(base, 2)
    shuffle_key = jax.random.fold_in(base, 3)
    hot = jax.random.randint(hot_key, (GROUPS,), 0, FINE)
    perms = jax.vmap(lambda sub: jax.random.permutation(sub, FINE))(jax.random.split(perm_key, blocks * GROUPS))
    perms = perms.reshape(blocks, GROUPS, FINE).astype(jnp.int32)
    raw = pattern[perms]
    column = jnp.arange(FINE, dtype=jnp.int32)
    top_pos = jnp.sum(column * (perms == 0).astype(jnp.int32), axis=-1)
    is_hot = column[None, None, :] == hot[None, :, None]
    raw_hot = jnp.sum(raw * is_hot.astype(jnp.int32), axis=-1, keepdims=True)
    weight = jnp.where(is_hot, 16, jnp.where(column[None, None, :] == top_pos[..., None], raw_hot, raw))
    counts = weight * CAP // 16
    bounds = jnp.cumsum(counts, axis=-1)
    within = jnp.arange(per_group, dtype=jnp.int32)
    first = jnp.sum((within[None, None, :, None] >= bounds[:, :, None, :]).astype(jnp.int32), axis=-1)
    second = jnp.sum(((within + per_group)[None, None, :, None] >= bounds[:, :, None, :]).astype(jnp.int32), axis=-1)
    group = jnp.broadcast_to(jnp.arange(GROUPS, dtype=jnp.int32)[None, :, None], first.shape)
    group = group.reshape(blocks, TOK_DEV)
    fine = jnp.stack([first, second], axis=-1).reshape(blocks, TOK_DEV, 2)
    shuffle = jax.vmap(lambda sub: jax.random.permutation(sub, TOK_DEV))(jax.random.split(shuffle_key, blocks)).astype(jnp.int32)
    group = jnp.take_along_axis(group, shuffle, axis=1)
    fine = jnp.take_along_axis(fine, shuffle[:, :, None], axis=1)
    return (group.reshape(TOKENS).astype(jnp.int32), fine.reshape(TOKENS, 2).astype(jnp.int32))


def draw_expert_group(key, part):
    return route_tables(key)[0]


def draw_expert_fine(key, part):
    return route_tables(key)[1]


def shard_levels(stream_key, extent, cuts, low, largest):
    loudness = 1.0
    for dim, parts in cuts:
        steps = jax.random.uniform(jax.random.fold_in(jax.random.fold_in(stream_key, 6), dim), (parts,), jnp.float32, low / len(cuts), largest / len(cuts))
        loudness = loudness * jnp.repeat(jnp.exp(steps), extent[dim] // parts).reshape((-1,) + (1,) * (len(extent) - 1 - dim))
    return loudness


def noise(rng, dims, deviation, most, cuts=(), held_as=jnp.bfloat16):
    loudness = shard_levels(rng, dims, cuts, -0.22, 0.18) if cuts else 1.0
    values = jax.random.normal(rng, dims, jnp.float32) * deviation * loudness
    return jnp.minimum(jnp.maximum(values, -most), most).astype(held_as)


def setup_inputs(seed: int = 0) -> dict:
    key_of = jax.random.split(jax.random.key(seed), 9)
    return {
        "tokens": noise(key_of[0], (TOKENS, D), 1.0, 6.0, ((0, 32),)),
        "expert_group": draw_expert_group(jax.random.fold_in(key_of[8], 71), 0),
        "expert_fine": draw_expert_fine(jax.random.fold_in(key_of[8], 71), 0),
        "route_weight": jnp.clip(0.2 + 0.7 * jax.random.uniform(key_of[3], (TOKENS, TOP), jnp.float32) ** shard_levels(key_of[3], (TOKENS, TOP), ((0, 32),), -0.2, 0.2), 0.2, 0.9),
        "norm_gain": jnp.clip(1.0 + 0.18 * jax.random.normal(key_of[4], (D,), jnp.float32), 0.1, 1.9),
        "gate_master": noise(key_of[5], (EXPERTS, D, F), D ** -0.5, 0.125, ((1, 8), (2, 4)), jnp.float32),
        "up_master": noise(key_of[6], (EXPERTS, D, F), D ** -0.5, 0.125, ((1, 8), (2, 4)), jnp.float32),
        "down_master": noise(key_of[7], (EXPERTS, D, F), F ** -0.5, 0.25, ((1, 8), (2, 4)), jnp.float32),
    }


EPS = 1e-06

def reference(tokens, expert_group, expert_fine, route_weight, norm_gain, gate_master, up_master, down_master):
    gate_ready = (norm_gain[None, :, None] * gate_master).astype(jnp.bfloat16)
    up_ready = (norm_gain[None, :, None] * up_master).astype(jnp.bfloat16)
    down_ready = down_master.astype(jnp.bfloat16)
    widened = tokens.astype(jnp.float32)
    normed = (widened * lax.rsqrt(lax.optimization_barrier(jnp.mean(widened * widened, axis=-1, keepdims=True)) + EPS)).astype(jnp.bfloat16)
    expert = (FINE * expert_group[:, None] + expert_fine).reshape(-1).astype(jnp.int32)
    weights = route_weight.reshape(-1)
    slot_count = DEVICES * CAP

    def per_expert(totals, expert_id):
        hits = expert == expert_id
        chosen = jnp.nonzero(hits, size=slot_count, fill_value=0)[0].astype(jnp.int32)
        filled = jnp.arange(slot_count, dtype=jnp.int32) < jnp.sum(hits.astype(jnp.int32))
        source_row = chosen // TOP
        input_rows = normed[source_row]
        gate_value = jnp.dot(input_rows, gate_ready[expert_id], preferred_element_type=jnp.float32)
        upward = jnp.dot(input_rows, up_ready[expert_id], preferred_element_type=jnp.float32)
        activation = (jax.nn.silu(gate_value) * upward).astype(jnp.bfloat16)
        produced = lax.dot_general(activation, down_ready[expert_id], (((1,), (1,)), ((), ())), preferred_element_type=jnp.float32).astype(jnp.bfloat16)
        scale = jnp.where(filled, weights[chosen], jnp.zeros((), weights.dtype)).astype(jnp.float32)
        totals = totals.at[source_row].add(scale[:, None] * produced.astype(jnp.float32))
        return (totals, None)
    totals, _ = lax.scan(per_expert, jnp.zeros((TOKENS, D), jnp.float32), jnp.arange(EXPERTS, dtype=jnp.int32))
    mixed = totals.astype(jnp.bfloat16)
    return (mixed, gate_ready, up_ready, down_ready)
```

```python
import functools

import jax
import jax.numpy as jnp
from jax import lax
from jax.experimental import pallas as pl
from jax.experimental.pallas import tpu as pltpu
from jax.sharding import PartitionSpec as P

FINE = 4


EPS = 1e-06


def flip(value, axis, bit):
    size = lax.axis_size(axis)
    return lax.ppermute(value, axis, [(i, i ^ bit) for i in range(size)])


def shift(value, axis, step):
    size = lax.axis_size(axis)
    return lax.ppermute(value, axis, [(i, (i + step) % size) for i in range(size)])


def gather_kernel(
    fs_size, tp_size, members, cap, tok_ref, piece_ref, x_ref, ready_ref,
    local_sem, tsend, trecv, psend, precv, xsend, xrecv, csend, crecv,
):
    groups, chips = fs_size // members, tp_size // 2
    tok_rows = tok_ref.shape[0]
    rows = piece_ref.shape[2]
    fs, tp = lax.axis_index("fs"), lax.axis_index("tp")
    group, member = fs // members, fs % members
    chip, core = tp // 2, tp % 2

    def away(r, i):
        base = member + i - 2 * (member & i)
        ahead = ((group + r) % groups) * members + base
        behind = ((group + groups - r) % groups) * members + base
        return ahead, behind

    def chip_tp(q, c):
        return ((chip + q) % chips) * 2 + c

    peers = [
        (away(r, i)[0], tp) for r in range(groups) for i in range(members) if r or i
    ]
    peers += [(fs, chip_tp(q, core)) for q in range(1, chips)] + [(fs, chip_tp(0, 1 - core))]
    barrier = pltpu.get_barrier_semaphore()
    for f, t in peers:
        pl.semaphore_signal(
            barrier, inc=1, device_id={"fs": f, "tp": t}, device_id_type=pl.DeviceIdType.MESH
        )
    pl.semaphore_wait(barrier, len(peers))

    started = []

    def send(src, dst, send_sem, recv_sem, f, t):
        copy = pltpu.make_async_remote_copy(
            src_ref=src, dst_ref=dst, send_sem=send_sem, recv_sem=recv_sem,
            device_id={"fs": f, "tp": t}, device_id_type=pl.DeviceIdType.MESH,
        )
        copy.start()
        started.append(copy)
        return copy

    near, far = pl.ds(0, cap), pl.ds(cap, tok_rows - cap)

    def pass_on(src, part, j, bit, k):
        return send(
            src, x_ref.at[j, part], tsend.at[k], trecv.at[k], away(0, bit)[0], tp
        )

    def block(f):
        return pl.ds(pl.multiple_of(f * rows, rows), rows)

    near_2 = pass_on(tok_ref.at[near], near, 2, 2, 0)
    near_1 = pass_on(tok_ref.at[near], near, 1, 1, 1)
    crossing = []
    for r in range(1, groups):
        part = pl.ds(r * cap, cap)
        crossing.append(
            send(tok_ref.at[part], x_ref.at[0, part], tsend.at[5 + r], trecv.at[5 + r], away(r, 0)[0], tp)
        )
    kept = pltpu.make_async_copy(tok_ref.at[near], x_ref.at[0, near], local_sem.at[0])
    kept.start()
    own = pltpu.make_async_copy(piece_ref.at[fs], ready_ref.at[tp, :, block(fs)], local_sem.at[1])
    own.start()

    pieces = {}
    for r in range(groups):
        for i in range(members):
            if r or i:
                k = r * members + i
                to = away(r, i)[0]
                pieces[r, i] = send(
                    piece_ref.at[to], ready_ref.at[tp, :, block(fs)], psend.at[k], precv.at[k], to, tp
                )
    own.wait()
    across = {}

    def cross_chips(r, i):
        here = ready_ref.at[tp, :, block(away(r, i)[1])]
        for q in range(1, chips):
            k = r * members + i
            across[q, r, i] = send(
                here, here, xsend.at[q - 1, k], xrecv.at[q - 1, k], fs, chip_tp(q, core)
            )

    beside = []

    def cross_cores(q, r):
        size = members * rows
        start = ((group + groups - r) % groups) * size
        here = ready_ref.at[chip_tp(chips - q, core), :, pl.ds(pl.multiple_of(start, size), size)]
        beside.append(
            send(here, here, csend.at[q, r], crecv.at[q, r], fs, chip_tp(0, 1 - core))
        )

    cross_chips(0, 0)
    for i in range(1, members):
        pieces[0, i].wait_recv()
        cross_chips(0, i)
    cross_cores(0, 0)
    near_2.wait_recv()
    near_3 = pass_on(x_ref.at[2, near], near, 3, 1, 2)
    for copy in crossing:
        copy.wait_recv()
    far_2 = pass_on(x_ref.at[0, far], far, 2, 2, 3)
    far_1 = pass_on(x_ref.at[0, far], far, 1, 1, 4)
    passed = False
    for r in range(1, groups):
        for i in range(members):
            pieces[r, i].wait_recv()
            cross_chips(r, i)
            if not passed and i == members // 2 - 1:
                passed = True
                far_2.wait_recv()
                far_3 = pass_on(x_ref.at[2, far], far, 3, 1, 5)
        cross_cores(0, r)
    for r in range(groups):
        for q in range(1, chips):
            for i in range(members):
                across[q, r, i].wait_recv()
            cross_cores(q, r)
    near_1.wait_recv()
    near_3.wait_recv()
    far_1.wait_recv()
    far_3.wait_recv()
    for copy in beside:
        copy.wait_recv()
    kept.wait()
    for copy in started:
        copy.wait_send()


def gather(ordered, pieces, members, cap):
    fs_size, tp_size = lax.axis_size("fs"), lax.axis_size("tp")
    experts_all, kinds, rows, cols = pieces.shape
    chips = tp_size // 2
    moves, crossings = 6, fs_size // members - 1
    dma = pltpu.SemaphoreType.DMA
    sent = 5 * ordered.size + 3 * pieces.size
    return pl.pallas_call(
        functools.partial(gather_kernel, fs_size, tp_size, members, cap),
        out_shape=(
            jax.ShapeDtypeStruct((members,) + ordered.shape, ordered.dtype),
            jax.ShapeDtypeStruct((tp_size, kinds, fs_size * rows, cols), pieces.dtype),
        ),
        in_specs=[pl.BlockSpec(memory_space=pltpu.VMEM)] * 2,
        out_specs=(pl.BlockSpec(memory_space=pl.ANY),) * 2,
        scratch_shapes=[
            dma((2,)),
            dma((moves + crossings,)),
            dma((moves + crossings,)),
            dma((fs_size,)),
            dma((fs_size,)),
            dma((max(chips - 1, 1), fs_size)),
            dma((max(chips - 1, 1), fs_size)),
            dma((chips, fs_size // members)),
            dma((chips, fs_size // members)),
        ],
        compiler_params=pltpu.CompilerParams(collective_id=0, has_side_effects=True),
        cost_estimate=pl.CostEstimate(flops=0, bytes_accessed=4 * sent, transcendentals=0),
    )(ordered, pieces)


def apply_rows(x_ref, mine_ref, gate_ref, up_ref, down_ref, kept_ref, sent_ref, kept_at, sent_at):
    members, cap, _ = x_ref.shape
    width, _ = gate_ref.shape
    x = x_ref[:, :, :width].reshape(members * cap, width)
    parts = x_ref[:, :, width:].reshape(members * cap, -1).astype(jnp.float32)
    weight = jnp.sum(parts * mine_ref[...], axis=1, keepdims=True)
    gate_value = jnp.dot(x, gate_ref[...], preferred_element_type=jnp.float32)
    upward = jnp.dot(x, up_ref[...], preferred_element_type=jnp.float32)
    activation = (gate_value / (1.0 + jnp.exp(-gate_value)) * upward).astype(jnp.bfloat16)
    step = min(width, 512)
    for at in range(0, width, step):
        out = lax.dot_general(
            activation,
            down_ref[at : at + step, :],
            (((1,), (1,)), ((), ())),
            preferred_element_type=jnp.float32,
        )
        out = (weight * out).astype(jnp.bfloat16)
        for ref, places in ((kept_ref, kept_at), (sent_ref, sent_at)):
            for i, j in enumerate(places):
                ref[i, :, at : at + step] = out[j * cap : (j + 1) * cap]


def first_kernel(kept_at, sent_at, x_ref, mine_ref, ready_ref, kept_ref, sent_ref, *whole_refs):
    @pl.when(pl.program_id(0) == 0)
    def _():
        cols = ready_ref.shape[3]
        for kind, ref in enumerate(whole_refs):
            for t in range(ready_ref.shape[0]):
                ref[0, :, t * cols : (t + 1) * cols] = ready_ref[t, kind]

    apply_rows(
        x_ref, mine_ref, *(ref.at[0] for ref in whole_refs), kept_ref, sent_ref, kept_at, sent_at
    )


def second_kernel(kept_at, sent_at, x_ref, mine_ref, gate_ref, up_ref, down_ref, kept_ref, sent_ref):
    apply_rows(
        x_ref, mine_ref, gate_ref.at[0], up_ref.at[0], down_ref.at[0],
        kept_ref, sent_ref, kept_at, sent_at,
    )


def expert_rows(x_all, mine, weights, cap, first_block, blocks, kept_at, sent_at):
    members, _, extended = x_all.shape
    gathered = len(weights) == 1
    if gathered:
        tp_size, kinds, width, cols = weights[0].shape
        whole = (1, width, tp_size * cols)
    else:
        whole = weights[0].shape
        width = whole[1]

    def fixed(shape):
        return pl.BlockSpec(shape, lambda i: (0,) * len(shape))

    half = jax.ShapeDtypeStruct((members // 2, blocks * cap, width), jnp.bfloat16)
    half_spec = pl.BlockSpec((members // 2, cap, width), lambda i: (0, i, 0))
    extra = 3 if gathered else 0
    body = functools.partial(first_kernel if gathered else second_kernel, kept_at, sent_at)
    hidden = whole[2]
    return pl.pallas_call(
        body,
        grid=(blocks,),
        in_specs=[
            pl.BlockSpec((members, cap, extended), lambda i: (0, i + first_block, 0)),
            fixed(mine.shape),
        ]
        + [fixed(w.shape) for w in weights],
        out_specs=[half_spec] * 2 + [fixed(whole)] * extra,
        out_shape=[half] * 2 + [jax.ShapeDtypeStruct(whole, jnp.bfloat16)] * extra,
        compiler_params=pltpu.CompilerParams(vmem_limit_bytes=56 << 20),
        cost_estimate=pl.CostEstimate(
            flops=6 * members * blocks * cap * width * hidden,
            bytes_accessed=2 * (6 * width * hidden + 2 * members * blocks * cap * width),
            transcendentals=members * blocks * cap * hidden,
        ),
    )(x_all, mine, *weights)


def local(
    tokens, expert_group, expert_fine, route_weight, norm_gain, gate_master, up_master, down_master
):
    tok_rows, width = tokens.shape
    fs_size = lax.axis_size("fs")
    experts_all = gate_master.shape[0]
    groups = experts_all // FINE
    members = fs_size // groups
    cap = tok_rows // groups
    fs_me = lax.axis_index("fs")
    group_me, fine_me = fs_me // members, fs_me % members

    widened = tokens.astype(jnp.float32)
    normed = (
        widened * lax.rsqrt(jnp.mean(widened * widened, axis=-1, keepdims=True) + EPS)
    ).astype(jnp.bfloat16)
    away = (expert_group - group_me + groups) % groups
    index = jnp.arange(tok_rows, dtype=jnp.int32)
    same = (away[:, None] == away[None, :]) & (index[None, :] < index[:, None])
    slot = away * cap + jnp.sum(same.astype(jnp.int32), axis=1)
    placing = (index[:, None] == slot[None, :]).astype(jnp.bfloat16)
    fines = jnp.arange(FINE, dtype=jnp.int32)
    share = jnp.sum(
        jnp.where(expert_fine[:, None, :] == fines[None, :, None], route_weight[:, None, :], 0.0),
        axis=2,
    )
    high = lax.reduce_precision(share, 8, 7)
    middle = lax.reduce_precision(share - high, 8, 7)
    low = share - high - middle
    terms = jnp.concatenate([high, middle, low], axis=1).astype(jnp.bfloat16)
    terms = jnp.pad(terms, ((0, 0), (0, 128 - terms.shape[1])))
    extended = jnp.concatenate([normed, terms], axis=1)
    ordered = jnp.dot(placing, extended, preferred_element_type=jnp.float32).astype(jnp.bfloat16)

    pieces = jnp.stack(
        [norm_gain[None, :, None] * gate_master, norm_gain[None, :, None] * up_master, down_master],
        axis=1,
    ).astype(jnp.bfloat16)
    x_all, ready = gather(ordered, pieces, members, cap)
    lanes = jnp.arange(128, dtype=jnp.int32)
    mine = ((lanes % FINE == fine_me) & (lanes < 3 * FINE)).astype(jnp.float32)[None, :]

    def collect(kept, sent, first, second):
        far_part = flip(sent, "fs", second)
        pair = (kept.astype(jnp.float32) + far_part.astype(jnp.float32)).astype(jnp.bfloat16)
        back = flip(pair[1], "fs", first)
        return (pair[0].astype(jnp.float32) + back.astype(jnp.float32)).astype(jnp.bfloat16)

    kept, sent, gate_ready, up_ready, down_ready = expert_rows(
        x_all, mine, (ready,), cap, 1, groups - 1, (0, 2), (1, 3)
    )
    far_mixed = collect(kept, sent, 2, 1)
    kept, sent = expert_rows(
        x_all, mine, (gate_ready, up_ready, down_ready), cap, 0, 1, (0, 1), (2, 3)
    )
    near_mixed = collect(kept, sent, 1, 2)
    returned = [near_mixed] + [
        shift(far_mixed[(r - 1) * cap : r * cap], "fs", -r * members) for r in range(1, groups)
    ]
    mixed = lax.dot_general(
        placing,
        jnp.concatenate(returned),
        (((0,), (0,)), ((), ())),
        preferred_element_type=jnp.float32,
    ).astype(jnp.bfloat16)
    return (mixed, gate_ready, up_ready, down_ready)


def fused_kernel(
    groups, chips, cap, gain_ref, group_ref, fine_ref, weight_ref, tok_hbm, gate_hbm, up_hbm, down_hbm,
    mixed_ref, gate_out, up_out, down_out,
    master, tok, piece_gu, piece_dn, w_gu, w_dn, x_rows, far_rows, share, far_share, act,
    y_send, y_recv, part, z_send, ret, place,
    lsem, gsend, grecv, dsend, drecv, tsend, trecv, ysend, yrecv, zsend, zrecv,
):
    rows, cols = piece_gu.shape[4:]
    toks, width = tok.shape
    hidden = w_dn.shape[2]
    fs, tp = lax.axis_index("fs"), lax.axis_index("tp")
    group, bit, side = fs // FINE, (fs // 2) % 2, fs % 2
    chip, core = tp // 2, tp % 2
    bf16, f32 = jnp.bfloat16, jnp.float32

    def ahead(r):
        return (group + r) % groups

    def behind(r):
        return (group + groups - r) % groups

    def member(grp, bb, jj):
        return grp * FINE + (bit + bb - 2 * bit * bb) * 2 + (side + jj - 2 * side * jj)

    def chip_ahead(q):
        return (chip + q) % chips

    def chip_behind(q):
        return (chip + chips - q) % chips

    def block(f):
        return pl.ds(pl.multiple_of(f * rows, rows), rows)

    def lanes(t):
        return pl.ds(pl.multiple_of(t * cols, cols), cols)

    loads = []
    for k, (src, dst) in enumerate(
        ((gate_hbm, master.at[0]), (up_hbm, master.at[1]), (tok_hbm, tok), (down_hbm, master.at[2]))
    ):
        copy = pltpu.make_async_copy(src, dst, lsem.at[k])
        copy.start()
        loads.append(copy)

    links = [(member(ahead(r), 0, jj), tp) for r in range(groups) for jj in (0, 1) if r or jj]
    links += [(member(group, 1, 0), tp)]
    links += [(fs, chip_ahead(q) * 2 + core) for q in range(1, chips)] + [(fs, chip * 2 + 1 - core)]
    barrier = pltpu.get_barrier_semaphore()
    for f, t in links:
        pl.semaphore_signal(
            barrier, inc=1, device_id={"fs": f, "tp": t}, device_id_type=pl.DeviceIdType.MESH
        )

    started = []

    def send(src, dst, send_sem, recv_sem, f, t):
        copy = pltpu.make_async_remote_copy(
            src_ref=src, dst_ref=dst, send_sem=send_sem, recv_sem=recv_sem,
            device_id={"fs": f, "tp": t}, device_id_type=pl.DeviceIdType.MESH,
        )
        copy.start()
        started.append(copy)
        return copy

    gain = jnp.transpose(jnp.broadcast_to(gain_ref[...], (cols, rows)))
    loads[0].wait()
    loads[1].wait()
    experts_all = master.shape[1]
    for e in range(experts_all):
        for kind in (0, 1):
            piece_gu[e // FINE, e % 2, (e % FINE) // 2, kind] = (gain * master[kind, e]).astype(bf16)
    pl.semaphore_wait(barrier, len(links))

    class Route:
        def __init__(self, piece, whole, send_sem, recv_sem):
            self.piece, self.whole, self.lead = piece, whole, (slice(None),) * (len(whole.shape) - 2)
            self.send_sem, self.recv_sem = send_sem, recv_sem
            self.count = 0
            self.got = {}

        def region(self, f, t):
            return self.whole.at[self.lead + (block(f), lanes(t))]

        def go(self, src, dst, f, t):
            k = self.count
            self.count += 1
            return send(src, dst, self.send_sem.at[k], self.recv_sem.at[k], f, t)

        def src(self, r, bb, jj):
            if r or bb or jj:
                return self.region(member(behind(r), bb, jj), tp)
            return self.piece.at[group, side]

        def direct(self, r, jj):
            to = member(ahead(r), 0, jj)
            j = side + jj - 2 * side * jj
            self.got[r, 0, jj] = self.go(self.piece.at[ahead(r), j], self.region(fs, tp), to, tp)

        def relay(self, r, jj):
            here = self.region(member(behind(r), 0, jj), tp)
            self.got[r, 1, jj] = self.go(self.src(r, 0, jj), here, member(group, 1, 0), tp)

        def across(self, r, bb, jj):
            here = self.region(member(behind(r), bb, jj), tp)
            for q in range(1, chips):
                self.got[r, bb, jj, q] = self.go(
                    self.src(r, bb, jj), here, fs, chip_ahead(q) * 2 + core
                )

        def beside(self, r, bb, jj, q):
            here = self.region(member(behind(r), bb, jj), chip_behind(q) * 2 + core)
            src = self.src(r, bb, jj) if q == 0 else here
            self.got[r, bb, jj, "core", q] = self.go(src, here, fs, chip * 2 + 1 - core)

        def wait(self, *key):
            self.got[key].wait_recv()

    gu = Route(piece_gu, w_gu, gsend, grecv)
    dn = Route(piece_dn, w_dn, dsend, drecv)

    gu.direct(0, 1)
    gu.relay(0, 0)
    gu.across(0, 0, 0)
    for r in range(1, groups):
        gu.direct(r, 0)
        gu.direct(r, 1)
    gu.beside(0, 0, 0, 0)
    keep_gu = pltpu.make_async_copy(piece_gu.at[group, side], gu.region(fs, tp), lsem.at[4])
    keep_gu.start()

    loads[2].wait()
    pad = max(8, groups)
    away = group_ref[...] - group
    away = jnp.where(away < 0, away + groups, away)
    which = lax.broadcasted_iota(jnp.int32, (pad, toks), 0)
    mine = (which == away).astype(f32)
    first = lax.broadcasted_iota(jnp.int32, (toks, toks), 0)
    second = lax.broadcasted_iota(jnp.int32, (toks, toks), 1)
    before = jnp.dot(
        mine.astype(bf16), (first < second).astype(f32).astype(bf16), preferred_element_type=f32
    )
    slot = jnp.sum(mine * (before + (which * cap).astype(f32)), axis=0, keepdims=True)
    placing = (first.astype(f32) == slot).astype(f32)
    place[...] = placing.astype(bf16)
    finer = lax.broadcasted_iota(jnp.int32, (8, toks), 0)
    shares = jnp.zeros((8, toks), f32)
    for k in range(fine_ref.shape[0]):
        shares += jnp.where(finer == fine_ref[k : k + 1, :], weight_ref[k : k + 1, :], 0.0)
    shares = lax.dot_general(
        shares, placing, (((1,), (1,)), ((), ())),
        preferred_element_type=f32, precision=lax.Precision.HIGHEST,
    )

    def normed(r):
        raw = jnp.dot(place[r * cap : (r + 1) * cap, :], tok[...], preferred_element_type=f32)
        scale = lax.rsqrt(jnp.mean(raw * raw, axis=1, keepdims=True) + EPS)
        return (raw * scale).astype(bf16)

    def at(r, jj):
        return pl.ds((r * 2 + jj) * cap, cap)

    share[0, 0] = shares[:, :cap]
    for r in range(1, groups):
        far_share[r - 1] = shares[:, r * cap : (r + 1) * cap]
    x_rows[at(0, 0), :] = normed(0)
    mate = member(group, 0, 1)
    arrivals, token_count = {}, [0]

    def send_rows(src, dst, f):
        k = token_count[0]
        token_count[0] += 1
        return send(src, dst, tsend.at[k], trecv.at[k], f, tp)

    arrivals["share", 0, 1] = send_rows(share.at[0, 0], share.at[0, 1], mate)
    arrivals["near"] = send_rows(x_rows.at[at(0, 0)], x_rows.at[at(0, 1)], mate)
    parts = 2
    step = cap // parts
    for r in range(1, groups):
        far_rows[r - 1] = normed(r)
        to = member(ahead(r), 0, 0)
        arrivals["share", r, 0] = send_rows(far_share.at[r - 1], share.at[r, 0], to)
        for p in range(parts):
            arrivals["far", r, p] = send_rows(
                far_rows.at[r - 1, pl.ds(p * step, step)],
                x_rows.at[pl.ds(r * 2 * cap + p * step, step)], to,
            )

    loads[3].wait()
    for e in range(experts_all):
        piece_dn[e // FINE, e % 2, (e % FINE) // 2] = master[2, e].astype(bf16)
    dn.direct(0, 1)
    for r in range(1, groups):
        dn.direct(r, 0)
        dn.direct(r, 1)
    dn.beside(0, 0, 0, 0)
    keep_dn = pltpu.make_async_copy(piece_dn.at[group, side], dn.region(fs, tp), lsem.at[5])
    keep_dn.start()

    def arrived(route, r, bb, jj):
        route.wait(r, bb, jj)
        if not bb:
            route.relay(r, jj)
        route.across(r, bb, jj)
        route.beside(r, bb, jj, 0)

    order = [(0, 0, 0), (0, 0, 1), (0, 1, 0)]
    for r in range(1, groups):
        order += [(r, 0, 0), (r - 1, 1, 1), (r, 0, 1), (r, 1, 0)]
    order += [(groups - 1, 1, 1)]
    for key in order[1:]:
        arrived(gu, *key)

    dn.relay(0, 0)
    dn.across(0, 0, 0)
    for key in ((0, 0, 1), (0, 1, 0), (0, 1, 1)):
        arrived(dn, *key)

    def apply_rows(start, count, s, lane0, lane_count):
        here = pl.ds(start * cap, count * cap)
        x = x_rows[here, :]
        at_lanes = pl.ds(pl.multiple_of(lane0, cols), lane_count)
        gate_value = jnp.dot(x, w_gu[s, 0, :, at_lanes], preferred_element_type=f32)
        upward = jnp.dot(x, w_gu[s, 1, :, at_lanes], preferred_element_type=f32)
        fine = s * 2 + side
        chosen = []
        for i in range(start, start + count):
            flat = jnp.transpose(share[i // 2, i % 2])
            lane = lax.broadcasted_iota(jnp.int32, flat.shape, 1)
            chosen.append(jnp.sum(jnp.where(lane == fine, flat, 0.0), axis=1, keepdims=True))
        weight = jnp.concatenate(chosen, axis=0)
        value = gate_value / (1.0 + jnp.exp(-gate_value)) * upward * weight
        act[here, pl.ds(pl.multiple_of(s * hidden + lane0, cols), lane_count)] = value.astype(bf16)

    keep_gu.wait()
    for key in order:
        gu.wait(*key, "core", 0)
    arrivals["share", 0, 1].wait_recv()
    arrivals["near"].wait_recv()
    pair = 2 * cols
    for s in (0, 1):
        apply_rows(0, 2, s, chip * pair, pair)

    tail = 3
    for key in order[:-tail]:
        for q in range(1, chips):
            gu.wait(*key, q)
            gu.beside(*key, q)
    for r in range(1, groups):
        arrivals["share", r, 0].wait_recv()
        arrivals["share", r, 1] = send_rows(share.at[r, 0], share.at[r, 1], mate)
        for p in range(parts):
            arrivals["far", r, p].wait_recv()
            arrivals["pass", r, p] = send_rows(
                x_rows.at[pl.ds(r * 2 * cap + p * step, step)],
                x_rows.at[pl.ds((r * 2 + 1) * cap + p * step, step)], mate,
            )
    for key in order[-tail:]:
        for q in range(1, chips):
            gu.wait(*key, q)
            gu.beside(*key, q)
    for key in order:
        for q in range(1, chips):
            gu.wait(*key, "core", q)
    for q in range(1, chips):
        for s in (0, 1):
            apply_rows(0, 2, s, chip_behind(q) * pair, pair)
    outs = [
        pltpu.make_async_copy(w_gu.at[bit, 0], gate_out.at[0], lsem.at[6]),
        pltpu.make_async_copy(w_gu.at[bit, 1], up_out.at[0], lsem.at[7]),
    ]
    for copy in outs:
        copy.start()
    for r in range(1, groups):
        for jj in (0, 1):
            arrived(dn, r, 0, jj)
    for r in range(1, groups):
        arrivals["share", r, 1].wait_recv()
        for p in range(parts):
            arrivals["pass", r, p].wait_recv()
        for s in (0, 1):
            for half in range(chips):
                apply_rows(2 * r, 2, s, half * pair, pair)
        for jj in (0, 1):
            arrived(dn, r, 1, jj)

    keep_dn.wait()
    span = 2 * rows
    steps = [(r, bb) for r in range(groups) for bb in (0, 1)]

    def columns(n):
        r, bb = steps[n]
        start = (behind(r) * FINE + (bit + bb - 2 * bit * bb) * 2) * rows
        return pl.ds(pl.multiple_of(start, span), span)

    crossing, home = {}, {}

    def produce(n):
        r, bb = steps[n]
        keys = [(r, bb, 0), (r, bb, 1)]
        for key in keys:
            for q in range(1, chips):
                dn.wait(*key, q)
                dn.beside(*key, q)
        for key in keys:
            for q in range(chips):
                dn.wait(*key, "core", q)
        here = columns(n)
        for r in reversed(range(groups)):
            mine = pl.ds(r * 2 * cap, 2 * cap)
            out = jnp.zeros((2 * cap, span), f32)
            for s in (0, 1):
                out += lax.dot_general(
                    act[mine, s * hidden : (s + 1) * hidden], w_dn[s, here, :],
                    (((1,), (1,)), ((), ())), preferred_element_type=f32,
                )
            y_send[r, :, here] = out[cap:].astype(bf16)
            part[r, :, here] = out[:cap]
            k = n * groups + r
            crossing[n, r] = send(
                y_send.at[r, :, here], y_recv.at[r, :, here], ysend.at[k], yrecv.at[k], mate, tp
            )

    def combine(n):
        here = columns(n)
        for r in reversed(range(groups)):
            crossing[n, r].wait_recv()
            total = (part[r, :, here] + y_recv[r, :, here].astype(f32)).astype(bf16)
            if r == 0:
                ret[0, :, here] = total
            else:
                z_send[r - 1, :, here] = total
                k = n * (groups - 1) + r - 1
                home[n, r] = send(
                    z_send.at[r - 1, :, here], ret.at[r, :, here], zsend.at[k], zrecv.at[k],
                    member(behind(r), 0, 0), tp,
                )

    for n in range(len(steps)):
        produce(n)
        if n:
            combine(n - 1)
    outs.append(pltpu.make_async_copy(w_dn.at[bit], down_out.at[0], lsem.at[8]))
    outs[-1].start()
    combine(len(steps) - 1)
    for copy in home.values():
        copy.wait_recv()
    chunk = min(width, 512)
    for c in range(0, width, chunk):
        mixed_ref[:, c : c + chunk] = lax.dot_general(
            place[...],
            jnp.concatenate([ret[r, :, c : c + chunk] for r in range(groups)], axis=0),
            (((0,), (0,)), ((), ())),
            preferred_element_type=f32,
        ).astype(bf16)
    for copy in outs:
        copy.wait()
    for copy in started:
        copy.wait_send()


def fused(
    tokens, expert_group, expert_fine, route_weight, norm_gain, gate_master, up_master, down_master
):
    toks, width = tokens.shape
    fs_size, tp_size = lax.axis_size("fs"), lax.axis_size("tp")
    experts_all, rows, cols = gate_master.shape
    groups, chips, hidden = experts_all // FINE, tp_size // 2, cols * tp_size
    cap = toks // groups
    bf16, f32 = jnp.bfloat16, jnp.float32
    sources = groups * 4
    sends = 2 * groups - 1 + 2 * groups + sources * (chips - 1) + sources * chips
    moves = 2 + (groups - 1) * 6
    steps = 2 * groups
    vmem, dma = pltpu.VMEM, pltpu.SemaphoreType.DMA
    anywhere = pl.BlockSpec(memory_space=pl.ANY)
    local_spec = pl.BlockSpec(memory_space=pltpu.VMEM)
    whole = jax.ShapeDtypeStruct((1, width, hidden), bf16)
    sent = 2 * (3 * width * hidden * 2 + 6 * toks * width)
    return pl.pallas_call(
        functools.partial(fused_kernel, groups, chips, cap),
        out_shape=(jax.ShapeDtypeStruct((toks, width), bf16), whole, whole, whole),
        in_specs=[local_spec] * 4 + [anywhere] * 4,
        out_specs=(local_spec, anywhere, anywhere, anywhere),
        scratch_shapes=[
            vmem((3, experts_all, rows, cols), f32),
            vmem((toks, width), bf16),
            vmem((groups, 2, 2, 2, rows, cols), bf16),
            vmem((groups, 2, 2, rows, cols), bf16),
            vmem((2, 2, width, hidden), bf16),
            vmem((2, width, hidden), bf16),
            vmem((2 * groups * cap, width), bf16),
            vmem((groups - 1, cap, width), bf16),
            vmem((groups, 2, 8, cap), f32),
            vmem((groups - 1, 8, cap), f32),
            vmem((2 * groups * cap, 2 * hidden), bf16),
            vmem((groups, cap, width), bf16),
            vmem((groups, cap, width), bf16),
            vmem((groups, cap, width), f32),
            vmem((groups - 1, cap, width), bf16),
            vmem((groups, cap, width), bf16),
            vmem((toks, toks), bf16),
            dma((9,)),
            dma((sends,)), dma((sends,)), dma((sends,)), dma((sends,)),
            dma((moves,)), dma((moves,)),
            dma((steps * groups,)), dma((steps * groups,)),
            dma((steps * (groups - 1),)), dma((steps * (groups - 1),)),
        ],
        compiler_params=pltpu.CompilerParams(
            collective_id=1, has_side_effects=True, vmem_limit_bytes=56 << 20
        ),
        cost_estimate=pl.CostEstimate(
            flops=12 * groups * cap * 2 * width * hidden, bytes_accessed=sent, transcendentals=0
        ),
    )(
        norm_gain[None, :], expert_group[None, :], expert_fine.T, route_weight.T,
        tokens, gate_master, up_master, down_master,
    )


def step(*args):
    tp_size = lax.axis_size("tp")
    gate_master = args[5]
    groups = gate_master.shape[0] // FINE
    if lax.axis_size("fs") == gate_master.shape[0] and tp_size > 2 and groups > 1 and gate_master.shape[2] % 128 == 0:
        return fused(*args)
    return local(*args)


def solution(mesh):
    in_specs = (
        P(("fs", "tp"), None),
        P(("fs", "tp")),
        P(("fs", "tp"), None),
        P(("fs", "tp"), None),
        P("fs"),
        P(None, "fs", "tp"),
        P(None, "fs", "tp"),
        P(None, "fs", "tp"),
    )
    out_specs = (
        P(("fs", "tp"), None),
        P("fs", None, None),
        P("fs", None, None),
        P("fs", None, None),
    )
    return jax.shard_map(step, mesh=mesh, in_specs=in_specs, out_specs=out_specs, check_vma=False)
```

```python
import functools

import jax
import jax.numpy as jnp
from jax import lax
from jax.experimental import pallas as pl
from jax.experimental.pallas import tpu as pltpu
from jax.sharding import PartitionSpec as P

FINE = 4


EPS = 1e-06


def flip(value, axis, bit):
    size = lax.axis_size(axis)
    return lax.ppermute(value, axis, [(i, i ^ bit) for i in range(size)])


def shift(value, axis, step):
    size = lax.axis_size(axis)
    return lax.ppermute(value, axis, [(i, (i + step) % size) for i in range(size)])


def gather_kernel(
    fs_size, tp_size, members, cap, tok_ref, piece_ref, x_ref, ready_ref,
    local_sem, tsend, trecv, psend, precv, xsend, xrecv, csend, crecv,
):
    groups, chips = fs_size // members, tp_size // 2
    tok_rows = tok_ref.shape[0]
    rows = piece_ref.shape[2]
    fs, tp = lax.axis_index("fs"), lax.axis_index("tp")
    group, member = fs // members, fs % members
    chip, core = tp // 2, tp % 2

    def away(r, i):
        base = member + i - 2 * (member & i)
        ahead = ((group + r) % groups) * members + base
        behind = ((group + groups - r) % groups) * members + base
        return ahead, behind

    def chip_tp(q, c):
        return ((chip + q) % chips) * 2 + c

    peers = [
        (away(r, i)[0], tp) for r in range(groups) for i in range(members) if r or i
    ]
    peers += [(fs, chip_tp(q, core)) for q in range(1, chips)] + [(fs, chip_tp(0, 1 - core))]
    barrier = pltpu.get_barrier_semaphore()
    for f, t in peers:
        pl.semaphore_signal(
            barrier, inc=1, device_id={"fs": f, "tp": t}, device_id_type=pl.DeviceIdType.MESH
        )
    pl.semaphore_wait(barrier, len(peers))

    started = []

    def send(src, dst, send_sem, recv_sem, f, t):
        copy = pltpu.make_async_remote_copy(
            src_ref=src, dst_ref=dst, send_sem=send_sem, recv_sem=recv_sem,
            device_id={"fs": f, "tp": t}, device_id_type=pl.DeviceIdType.MESH,
        )
        copy.start()
        started.append(copy)
        return copy

    near, far = pl.ds(0, cap), pl.ds(cap, tok_rows - cap)

    def pass_on(src, part, j, bit, k):
        return send(
            src, x_ref.at[j, part], tsend.at[k], trecv.at[k], away(0, bit)[0], tp
        )

    def block(f):
        return pl.ds(pl.multiple_of(f * rows, rows), rows)

    near_2 = pass_on(tok_ref.at[near], near, 2, 2, 0)
    near_1 = pass_on(tok_ref.at[near], near, 1, 1, 1)
    crossing = []
    for r in range(1, groups):
        part = pl.ds(r * cap, cap)
        crossing.append(
            send(tok_ref.at[part], x_ref.at[0, part], tsend.at[5 + r], trecv.at[5 + r], away(r, 0)[0], tp)
        )
    kept = pltpu.make_async_copy(tok_ref.at[near], x_ref.at[0, near], local_sem.at[0])
    kept.start()
    own = pltpu.make_async_copy(piece_ref.at[fs], ready_ref.at[tp, :, block(fs)], local_sem.at[1])
    own.start()

    pieces = {}
    for r in range(groups):
        for i in range(members):
            if r or i:
                k = r * members + i
                to = away(r, i)[0]
                pieces[r, i] = send(
                    piece_ref.at[to], ready_ref.at[tp, :, block(fs)], psend.at[k], precv.at[k], to, tp
                )
    own.wait()
    across = {}

    def cross_chips(r, i):
        here = ready_ref.at[tp, :, block(away(r, i)[1])]
        for q in range(1, chips):
            k = r * members + i
            across[q, r, i] = send(
                here, here, xsend.at[q - 1, k], xrecv.at[q - 1, k], fs, chip_tp(q, core)
            )

    beside = []

    def cross_cores(q, r):
        size = members * rows
        start = ((group + groups - r) % groups) * size
        here = ready_ref.at[chip_tp(chips - q, core), :, pl.ds(pl.multiple_of(start, size), size)]
        beside.append(
            send(here, here, csend.at[q, r], crecv.at[q, r], fs, chip_tp(0, 1 - core))
        )

    cross_chips(0, 0)
    for i in range(1, members):
        pieces[0, i].wait_recv()
        cross_chips(0, i)
    cross_cores(0, 0)
    near_2.wait_recv()
    near_3 = pass_on(x_ref.at[2, near], near, 3, 1, 2)
    for copy in crossing:
        copy.wait_recv()
    far_2 = pass_on(x_ref.at[0, far], far, 2, 2, 3)
    far_1 = pass_on(x_ref.at[0, far], far, 1, 1, 4)
    passed = False
    for r in range(1, groups):
        for i in range(members):
            pieces[r, i].wait_recv()
            cross_chips(r, i)
            if not passed and i == members // 2 - 1:
                passed = True
                far_2.wait_recv()
                far_3 = pass_on(x_ref.at[2, far], far, 3, 1, 5)
        cross_cores(0, r)
    for r in range(groups):
        for q in range(1, chips):
            for i in range(members):
                across[q, r, i].wait_recv()
            cross_cores(q, r)
    near_1.wait_recv()
    near_3.wait_recv()
    far_1.wait_recv()
    far_3.wait_recv()
    for copy in beside:
        copy.wait_recv()
    kept.wait()
    for copy in started:
        copy.wait_send()


def gather(ordered, pieces, members, cap):
    fs_size, tp_size = lax.axis_size("fs"), lax.axis_size("tp")
    experts_all, kinds, rows, cols = pieces.shape
    chips = tp_size // 2
    moves, crossings = 6, fs_size // members - 1
    dma = pltpu.SemaphoreType.DMA
    sent = 5 * ordered.size + 3 * pieces.size
    return pl.pallas_call(
        functools.partial(gather_kernel, fs_size, tp_size, members, cap),
        out_shape=(
            jax.ShapeDtypeStruct((members,) + ordered.shape, ordered.dtype),
            jax.ShapeDtypeStruct((tp_size, kinds, fs_size * rows, cols), pieces.dtype),
        ),
        in_specs=[pl.BlockSpec(memory_space=pltpu.VMEM)] * 2,
        out_specs=(pl.BlockSpec(memory_space=pl.ANY),) * 2,
        scratch_shapes=[
            dma((2,)),
            dma((moves + crossings,)),
            dma((moves + crossings,)),
            dma((fs_size,)),
            dma((fs_size,)),
            dma((max(chips - 1, 1), fs_size)),
            dma((max(chips - 1, 1), fs_size)),
            dma((chips, fs_size // members)),
            dma((chips, fs_size // members)),
        ],
        compiler_params=pltpu.CompilerParams(collective_id=0, has_side_effects=True),
        cost_estimate=pl.CostEstimate(flops=0, bytes_accessed=4 * sent, transcendentals=0),
    )(ordered, pieces)


def apply_rows(x_ref, mine_ref, gate_ref, up_ref, down_ref, kept_ref, sent_ref, kept_at, sent_at):
    members, cap, _ = x_ref.shape
    width, _ = gate_ref.shape
    x = x_ref[:, :, :width].reshape(members * cap, width)
    parts = x_ref[:, :, width:].reshape(members * cap, -1).astype(jnp.float32)
    weight = jnp.sum(parts * mine_ref[...], axis=1, keepdims=True)
    gate_value = jnp.dot(x, gate_ref[...], preferred_element_type=jnp.float32)
    upward = jnp.dot(x, up_ref[...], preferred_element_type=jnp.float32)
    activation = (gate_value / (1.0 + jnp.exp(-gate_value)) * upward).astype(jnp.bfloat16)
    step = min(width, 512)
    for at in range(0, width, step):
        out = lax.dot_general(
            activation,
            down_ref[at : at + step, :],
            (((1,), (1,)), ((), ())),
            preferred_element_type=jnp.float32,
        )
        out = (weight * out).astype(jnp.bfloat16)
        for ref, places in ((kept_ref, kept_at), (sent_ref, sent_at)):
            for i, j in enumerate(places):
                ref[i, :, at : at + step] = out[j * cap : (j + 1) * cap]


def first_kernel(kept_at, sent_at, x_ref, mine_ref, ready_ref, kept_ref, sent_ref, *whole_refs):
    @pl.when(pl.program_id(0) == 0)
    def _():
        cols = ready_ref.shape[3]
        for kind, ref in enumerate(whole_refs):
            for t in range(ready_ref.shape[0]):
                ref[0, :, t * cols : (t + 1) * cols] = ready_ref[t, kind]

    apply_rows(
        x_ref, mine_ref, *(ref.at[0] for ref in whole_refs), kept_ref, sent_ref, kept_at, sent_at
    )


def second_kernel(kept_at, sent_at, x_ref, mine_ref, gate_ref, up_ref, down_ref, kept_ref, sent_ref):
    apply_rows(
        x_ref, mine_ref, gate_ref.at[0], up_ref.at[0], down_ref.at[0],
        kept_ref, sent_ref, kept_at, sent_at,
    )


def expert_rows(x_all, mine, weights, cap, first_block, blocks, kept_at, sent_at):
    members, _, extended = x_all.shape
    gathered = len(weights) == 1
    if gathered:
        tp_size, kinds, width, cols = weights[0].shape
        whole = (1, width, tp_size * cols)
    else:
        whole = weights[0].shape
        width = whole[1]

    def fixed(shape):
        return pl.BlockSpec(shape, lambda i: (0,) * len(shape))

    half = jax.ShapeDtypeStruct((members // 2, blocks * cap, width), jnp.bfloat16)
    half_spec = pl.BlockSpec((members // 2, cap, width), lambda i: (0, i, 0))
    extra = 3 if gathered else 0
    body = functools.partial(first_kernel if gathered else second_kernel, kept_at, sent_at)
    hidden = whole[2]
    return pl.pallas_call(
        body,
        grid=(blocks,),
        in_specs=[
            pl.BlockSpec((members, cap, extended), lambda i: (0, i + first_block, 0)),
            fixed(mine.shape),
        ]
        + [fixed(w.shape) for w in weights],
        out_specs=[half_spec] * 2 + [fixed(whole)] * extra,
        out_shape=[half] * 2 + [jax.ShapeDtypeStruct(whole, jnp.bfloat16)] * extra,
        compiler_params=pltpu.CompilerParams(vmem_limit_bytes=56 << 20),
        cost_estimate=pl.CostEstimate(
            flops=6 * members * blocks * cap * width * hidden,
            bytes_accessed=2 * (6 * width * hidden + 2 * members * blocks * cap * width),
            transcendentals=members * blocks * cap * hidden,
        ),
    )(x_all, mine, *weights)


def local(
    tokens, expert_group, expert_fine, route_weight, norm_gain, gate_master, up_master, down_master
):
    tok_rows, width = tokens.shape
    fs_size = lax.axis_size("fs")
    experts_all = gate_master.shape[0]
    groups = experts_all // FINE
    members = fs_size // groups
    cap = tok_rows // groups
    fs_me = lax.axis_index("fs")
    group_me, fine_me = fs_me // members, fs_me % members

    widened = tokens.astype(jnp.float32)
    normed = (
        widened * lax.rsqrt(jnp.mean(widened * widened, axis=-1, keepdims=True) + EPS)
    ).astype(jnp.bfloat16)
    away = (expert_group - group_me + groups) % groups
    index = jnp.arange(tok_rows, dtype=jnp.int32)
    same = (away[:, None] == away[None, :]) & (index[None, :] < index[:, None])
    slot = away * cap + jnp.sum(same.astype(jnp.int32), axis=1)
    placing = (index[:, None] == slot[None, :]).astype(jnp.bfloat16)
    fines = jnp.arange(FINE, dtype=jnp.int32)
    share = jnp.sum(
        jnp.where(expert_fine[:, None, :] == fines[None, :, None], route_weight[:, None, :], 0.0),
        axis=2,
    )
    high = lax.reduce_precision(share, 8, 7)
    middle = lax.reduce_precision(share - high, 8, 7)
    low = share - high - middle
    terms = jnp.concatenate([high, middle, low], axis=1).astype(jnp.bfloat16)
    terms = jnp.pad(terms, ((0, 0), (0, 128 - terms.shape[1])))
    extended = jnp.concatenate([normed, terms], axis=1)
    ordered = jnp.dot(placing, extended, preferred_element_type=jnp.float32).astype(jnp.bfloat16)

    pieces = jnp.stack(
        [norm_gain[None, :, None] * gate_master, norm_gain[None, :, None] * up_master, down_master],
        axis=1,
    ).astype(jnp.bfloat16)
    x_all, ready = gather(ordered, pieces, members, cap)
    lanes = jnp.arange(128, dtype=jnp.int32)
    mine = ((lanes % FINE == fine_me) & (lanes < 3 * FINE)).astype(jnp.float32)[None, :]

    def collect(kept, sent, first, second):
        far_part = flip(sent, "fs", second)
        pair = (kept.astype(jnp.float32) + far_part.astype(jnp.float32)).astype(jnp.bfloat16)
        back = flip(pair[1], "fs", first)
        return (pair[0].astype(jnp.float32) + back.astype(jnp.float32)).astype(jnp.bfloat16)

    kept, sent, gate_ready, up_ready, down_ready = expert_rows(
        x_all, mine, (ready,), cap, 1, groups - 1, (0, 2), (1, 3)
    )
    far_mixed = collect(kept, sent, 2, 1)
    kept, sent = expert_rows(
        x_all, mine, (gate_ready, up_ready, down_ready), cap, 0, 1, (0, 1), (2, 3)
    )
    near_mixed = collect(kept, sent, 1, 2)
    returned = [near_mixed] + [
        shift(far_mixed[(r - 1) * cap : r * cap], "fs", -r * members) for r in range(1, groups)
    ]
    mixed = lax.dot_general(
        placing,
        jnp.concatenate(returned),
        (((0,), (0,)), ((), ())),
        preferred_element_type=jnp.float32,
    ).astype(jnp.bfloat16)
    return (mixed, gate_ready, up_ready, down_ready)


def fused_kernel(
    groups, chips, cap, gain_ref, group_ref, fine_ref, weight_ref, tok_hbm, gate_hbm, up_hbm, down_hbm,
    mixed_ref, gate_out, up_out, down_out,
    master, tok, piece_gu, piece_dn, w_gu, w_dn, x_rows, far_rows, share, far_share, act,
    y_send, y_recv, part, z_send, ret, place,
    lsem, gsend, grecv, dsend, drecv, tsend, trecv, ysend, yrecv, zsend, zrecv,
):
    rows, cols = piece_gu.shape[4:]
    toks, width = tok.shape
    hidden = w_dn.shape[2]
    fs, tp = lax.axis_index("fs"), lax.axis_index("tp")
    group, bit, side = fs // FINE, (fs // 2) % 2, fs % 2
    chip, core = tp // 2, tp % 2
    bf16, f32 = jnp.bfloat16, jnp.float32

    def ahead(r):
        return (group + r) % groups

    def behind(r):
        return (group + groups - r) % groups

    def member(grp, bb, jj):
        return grp * FINE + (bit + bb - 2 * bit * bb) * 2 + (side + jj - 2 * side * jj)

    def chip_ahead(q):
        return (chip + q) % chips

    def chip_behind(q):
        return (chip + chips - q) % chips

    def block(f):
        return pl.ds(pl.multiple_of(f * rows, rows), rows)

    def lanes(t):
        return pl.ds(pl.multiple_of(t * cols, cols), cols)

    loads = []
    for k, (src, dst) in enumerate(
        ((gate_hbm, master.at[0]), (up_hbm, master.at[1]), (tok_hbm, tok), (down_hbm, master.at[2]))
    ):
        copy = pltpu.make_async_copy(src, dst, lsem.at[k])
        copy.start()
        loads.append(copy)

    links = [(member(ahead(r), 0, jj), tp) for r in range(groups) for jj in (0, 1) if r or jj]
    links += [(member(group, 1, 0), tp)]
    links += [(fs, chip_ahead(q) * 2 + core) for q in range(1, chips)] + [(fs, chip * 2 + 1 - core)]
    barrier = pltpu.get_barrier_semaphore()
    for f, t in links:
        pl.semaphore_signal(
            barrier, inc=1, device_id={"fs": f, "tp": t}, device_id_type=pl.DeviceIdType.MESH
        )

    started = []

    def send(src, dst, send_sem, recv_sem, f, t):
        copy = pltpu.make_async_remote_copy(
            src_ref=src, dst_ref=dst, send_sem=send_sem, recv_sem=recv_sem,
            device_id={"fs": f, "tp": t}, device_id_type=pl.DeviceIdType.MESH,
        )
        copy.start()
        started.append(copy)
        return copy

    gain = jnp.transpose(jnp.broadcast_to(gain_ref[...], (cols, rows)))
    loads[0].wait()
    loads[1].wait()
    experts_all = master.shape[1]
    for e in range(experts_all):
        for kind in (0, 1):
            piece_gu[e // FINE, e % 2, (e % FINE) // 2, kind] = (gain * master[kind, e]).astype(bf16)
    pl.semaphore_wait(barrier, len(links))

    class Route:
        def __init__(self, piece, whole, send_sem, recv_sem):
            self.piece, self.whole, self.lead = piece, whole, (slice(None),) * (len(whole.shape) - 2)
            self.send_sem, self.recv_sem = send_sem, recv_sem
            self.count = 0
            self.got = {}

        def region(self, f, t):
            return self.whole.at[self.lead + (block(f), lanes(t))]

        def go(self, src, dst, f, t):
            k = self.count
            self.count += 1
            return send(src, dst, self.send_sem.at[k], self.recv_sem.at[k], f, t)

        def src(self, r, bb, jj):
            if r or bb or jj:
                return self.region(member(behind(r), bb, jj), tp)
            return self.piece.at[group, side]

        def direct(self, r, jj):
            to = member(ahead(r), 0, jj)
            j = side + jj - 2 * side * jj
            self.got[r, 0, jj] = self.go(self.piece.at[ahead(r), j], self.region(fs, tp), to, tp)

        def relay(self, r, jj):
            here = self.region(member(behind(r), 0, jj), tp)
            self.got[r, 1, jj] = self.go(self.src(r, 0, jj), here, member(group, 1, 0), tp)

        def across(self, r, bb, jj):
            here = self.region(member(behind(r), bb, jj), tp)
            for q in range(1, chips):
                self.got[r, bb, jj, q] = self.go(
                    self.src(r, bb, jj), here, fs, chip_ahead(q) * 2 + core
                )

        def beside(self, r, bb, jj, q):
            here = self.region(member(behind(r), bb, jj), chip_behind(q) * 2 + core)
            src = self.src(r, bb, jj) if q == 0 else here
            self.got[r, bb, jj, "core", q] = self.go(src, here, fs, chip * 2 + 1 - core)

        def wait(self, *key):
            self.got[key].wait_recv()

    gu = Route(piece_gu, w_gu, gsend, grecv)
    dn = Route(piece_dn, w_dn, dsend, drecv)

    gu.direct(0, 1)
    gu.relay(0, 0)
    gu.across(0, 0, 0)
    for r in range(1, groups):
        gu.direct(r, 0)
    gu.beside(0, 0, 0, 0)
    keep_gu = pltpu.make_async_copy(piece_gu.at[group, side], gu.region(fs, tp), lsem.at[4])
    keep_gu.start()

    loads[2].wait()
    pad = max(8, groups)
    away = group_ref[...] - group
    away = jnp.where(away < 0, away + groups, away)
    which = lax.broadcasted_iota(jnp.int32, (pad, toks), 0)
    mine = (which == away).astype(f32)
    first = lax.broadcasted_iota(jnp.int32, (toks, toks), 0)
    second = lax.broadcasted_iota(jnp.int32, (toks, toks), 1)
    before = jnp.dot(
        mine.astype(bf16), (first < second).astype(f32).astype(bf16), preferred_element_type=f32
    )
    slot = jnp.sum(mine * (before + (which * cap).astype(f32)), axis=0, keepdims=True)
    placing = (first.astype(f32) == slot).astype(f32)
    place[...] = placing.astype(bf16)
    finer = lax.broadcasted_iota(jnp.int32, (8, toks), 0)
    shares = jnp.zeros((8, toks), f32)
    for k in range(fine_ref.shape[0]):
        shares += jnp.where(finer == fine_ref[k : k + 1, :], weight_ref[k : k + 1, :], 0.0)
    shares = lax.dot_general(
        shares, placing, (((1,), (1,)), ((), ())),
        preferred_element_type=f32, precision=lax.Precision.HIGHEST,
    )

    def normed(r):
        raw = jnp.dot(place[r * cap : (r + 1) * cap, :], tok[...], preferred_element_type=f32)
        scale = lax.rsqrt(jnp.mean(raw * raw, axis=1, keepdims=True) + EPS)
        return (raw * scale).astype(bf16)

    def at(r, jj):
        return pl.ds((r * 2 + jj) * cap, cap)

    share[0, 0] = shares[:, :cap]
    for r in range(1, groups):
        far_share[r - 1] = shares[:, r * cap : (r + 1) * cap]
    x_rows[at(0, 0), :] = normed(0)
    mate = member(group, 0, 1)
    arrivals, token_count = {}, [0]

    def send_rows(src, dst, f):
        k = token_count[0]
        token_count[0] += 1
        return send(src, dst, tsend.at[k], trecv.at[k], f, tp)

    arrivals["share", 0, 1] = send_rows(share.at[0, 0], share.at[0, 1], mate)
    arrivals["near"] = send_rows(x_rows.at[at(0, 0)], x_rows.at[at(0, 1)], mate)
    for r in range(1, groups):
        far_rows[r - 1] = normed(r)
    parts = 2
    step = cap // parts

    def send_far(r):
        to = member(ahead(r), 0, 0)
        arrivals["share", r, 0] = send_rows(far_share.at[r - 1], share.at[r, 0], to)
        for p in range(parts):
            arrivals["far", r, p] = send_rows(
                far_rows.at[r - 1, pl.ds(p * step, step)],
                x_rows.at[pl.ds(r * 2 * cap + p * step, step)], to,
            )

    def pass_far(r):
        arrivals["share", r, 0].wait_recv()
        arrivals["share", r, 1] = send_rows(share.at[r, 0], share.at[r, 1], mate)
        for p in range(parts):
            arrivals["far", r, p].wait_recv()
            arrivals["pass", r, p] = send_rows(
                x_rows.at[pl.ds(r * 2 * cap + p * step, step)],
                x_rows.at[pl.ds((r * 2 + 1) * cap + p * step, step)], mate,
            )

    loads[3].wait()
    for e in range(experts_all):
        piece_dn[e // FINE, e % 2, (e % FINE) // 2] = master[2, e].astype(bf16)
    keep_dn = pltpu.make_async_copy(piece_dn.at[group, side], dn.region(fs, tp), lsem.at[5])
    keep_dn.start()

    def arrived(route, r, bb, jj):
        route.wait(r, bb, jj)
        if not bb:
            route.relay(r, jj)
        route.across(r, bb, jj)
        route.beside(r, bb, jj, 0)

    def crossed(route, r, bb, jj):
        for q in range(1, chips):
            route.wait(r, bb, jj, q)
            route.beside(r, bb, jj, q)

    order = [(0, 0, 0), (0, 0, 1), (0, 1, 0)]
    for r in range(1, groups):
        order += [(r, 0, 0), (r - 1, 1, 1), (r, 0, 1), (r, 1, 0)]
    order += [(groups - 1, 1, 1)]
    done = 0
    for k, key in enumerate(order[1:]):
        arrived(gu, *key)
        if key == (0, 0, 1):
            for r in range(1, groups):
                gu.direct(r, 1)
            dn.direct(0, 1)
            dn.beside(0, 0, 0, 0)
        if key[0] and key[1:] == (0, 1):
            send_far(key[0])
            dn.direct(key[0], 0)
            dn.direct(key[0], 1)
        if k >= 3:
            crossed(gu, *order[done])
            done += 1
    dn.relay(0, 0)
    dn.across(0, 0, 0)
    arrived(dn, 0, 0, 1)

    def apply_rows(start, count, s, lane0, lane_count):
        here = pl.ds(start * cap, count * cap)
        x = x_rows[here, :]
        at_lanes = pl.ds(pl.multiple_of(lane0, cols), lane_count)
        gate_value = jnp.dot(x, w_gu[s, 0, :, at_lanes], preferred_element_type=f32)
        upward = jnp.dot(x, w_gu[s, 1, :, at_lanes], preferred_element_type=f32)
        fine = s * 2 + side
        chosen = []
        for i in range(start, start + count):
            flat = jnp.transpose(share[i // 2, i % 2])
            lane = lax.broadcasted_iota(jnp.int32, flat.shape, 1)
            chosen.append(jnp.sum(jnp.where(lane == fine, flat, 0.0), axis=1, keepdims=True))
        weight = jnp.concatenate(chosen, axis=0)
        value = gate_value / (1.0 + jnp.exp(-gate_value)) * upward * weight
        act[here, pl.ds(pl.multiple_of(s * hidden + lane0, cols), lane_count)] = value.astype(bf16)

    keep_gu.wait()
    for key in order:
        gu.wait(*key, "core", 0)
    arrivals["share", 0, 1].wait_recv()
    arrivals["near"].wait_recv()
    pair = 2 * cols
    for s in (0, 1):
        apply_rows(0, 2, s, chip * pair, pair)

    for key in order[done:-1]:
        crossed(gu, *key)
    for r in range(1, groups):
        pass_far(r)
    crossed(gu, *order[-1])
    for key in order:
        for q in range(1, chips):
            gu.wait(*key, "core", q)
    for q in range(1, chips):
        for s in (0, 1):
            apply_rows(0, 2, s, chip_behind(q) * pair, pair)
    outs = [
        pltpu.make_async_copy(w_gu.at[bit, 0], gate_out.at[0], lsem.at[6]),
        pltpu.make_async_copy(w_gu.at[bit, 1], up_out.at[0], lsem.at[7]),
    ]
    for copy in outs:
        copy.start()

    keep_dn.wait()
    span = 2 * rows
    steps = [(r, bb) for r in range(groups) for bb in (0, 1)]

    def columns(n):
        r, bb = steps[n]
        start = (behind(r) * FINE + (bit + bb - 2 * bit * bb) * 2) * rows
        return pl.ds(pl.multiple_of(start, span), span)

    crossing, home = {}, {}

    def ready(n):
        r, bb = steps[n]
        keys = [(r, bb, 0), (r, bb, 1)]
        for key in keys:
            crossed(dn, *key)
        for key in keys:
            for q in range(chips):
                dn.wait(*key, "core", q)

    def produce(n, r):
        here = columns(n)
        mine = pl.ds(r * 2 * cap, 2 * cap)
        out = jnp.zeros((2 * cap, span), f32)
        for s in (0, 1):
            out += lax.dot_general(
                act[mine, s * hidden : (s + 1) * hidden], w_dn[s, here, :],
                (((1,), (1,)), ((), ())), preferred_element_type=f32,
            )
        y_send[r, :, here] = out[cap:].astype(bf16)
        part[r, :, here] = out[:cap]
        k = n * groups + r
        crossing[n, r] = send(
            y_send.at[r, :, here], y_recv.at[r, :, here], ysend.at[k], yrecv.at[k], mate, tp
        )

    def combine(n, r):
        here = columns(n)
        crossing[n, r].wait_recv()
        total = (part[r, :, here] + y_recv[r, :, here].astype(f32)).astype(bf16)
        if r == 0:
            ret[0, :, here] = total
        else:
            z_send[r - 1, :, here] = total
            k = n * (groups - 1) + r - 1
            home[n, r] = send(
                z_send.at[r - 1, :, here], ret.at[r, :, here], zsend.at[k], zrecv.at[k],
                member(behind(r), 0, 0), tp,
            )

    arrived(dn, 0, 1, 0)
    arrived(dn, 0, 1, 1)
    ready(0)
    produce(0, 0)
    for r in range(1, groups):
        for jj in (0, 1):
            arrived(dn, r, 0, jj)
    for r in range(1, groups):
        arrivals["share", r, 1].wait_recv()
        for p in range(parts):
            arrivals["pass", r, p].wait_recv()
        for s in (0, 1):
            for half in range(chips):
                apply_rows(2 * r, 2, s, half * pair, pair)
        produce(0, r)
    waiting = [(0, 0)] + [(0, r) for r in range(1, groups)]
    for n in range(1, len(steps)):
        if steps[n][0] and not steps[n][1]:
            for jj in (0, 1):
                arrived(dn, steps[n][0], 1, jj)
        ready(n)
        for r in reversed(range(groups)):
            produce(n, r)
            waiting.append((n, r))
            combine(*waiting.pop(0))
    outs.append(pltpu.make_async_copy(w_dn.at[bit], down_out.at[0], lsem.at[8]))
    outs[-1].start()
    for item in waiting:
        combine(*item)
    for copy in home.values():
        copy.wait_recv()
    chunk = min(width, 512)
    for c in range(0, width, chunk):
        mixed_ref[:, c : c + chunk] = lax.dot_general(
            place[...],
            jnp.concatenate([ret[r, :, c : c + chunk] for r in range(groups)], axis=0),
            (((0,), (0,)), ((), ())),
            preferred_element_type=f32,
        ).astype(bf16)
    for copy in outs:
        copy.wait()
    for copy in started:
        copy.wait_send()


def fused(
    tokens, expert_group, expert_fine, route_weight, norm_gain, gate_master, up_master, down_master
):
    toks, width = tokens.shape
    fs_size, tp_size = lax.axis_size("fs"), lax.axis_size("tp")
    experts_all, rows, cols = gate_master.shape
    groups, chips, hidden = experts_all // FINE, tp_size // 2, cols * tp_size
    cap = toks // groups
    bf16, f32 = jnp.bfloat16, jnp.float32
    sources = groups * 4
    sends = 2 * groups - 1 + 2 * groups + sources * (chips - 1) + sources * chips
    moves = 2 + (groups - 1) * 6
    steps = 2 * groups
    vmem, dma = pltpu.VMEM, pltpu.SemaphoreType.DMA
    anywhere = pl.BlockSpec(memory_space=pl.ANY)
    local_spec = pl.BlockSpec(memory_space=pltpu.VMEM)
    whole = jax.ShapeDtypeStruct((1, width, hidden), bf16)
    sent = 2 * (3 * width * hidden * 2 + 6 * toks * width)
    return pl.pallas_call(
        functools.partial(fused_kernel, groups, chips, cap),
        out_shape=(jax.ShapeDtypeStruct((toks, width), bf16), whole, whole, whole),
        in_specs=[local_spec] * 4 + [anywhere] * 4,
        out_specs=(local_spec, anywhere, anywhere, anywhere),
        scratch_shapes=[
            vmem((3, experts_all, rows, cols), f32),
            vmem((toks, width), bf16),
            vmem((groups, 2, 2, 2, rows, cols), bf16),
            vmem((groups, 2, 2, rows, cols), bf16),
            vmem((2, 2, width, hidden), bf16),
            vmem((2, width, hidden), bf16),
            vmem((2 * groups * cap, width), bf16),
            vmem((groups - 1, cap, width), bf16),
            vmem((groups, 2, 8, cap), f32),
            vmem((groups - 1, 8, cap), f32),
            vmem((2 * groups * cap, 2 * hidden), bf16),
            vmem((groups, cap, width), bf16),
            vmem((groups, cap, width), bf16),
            vmem((groups, cap, width), f32),
            vmem((groups - 1, cap, width), bf16),
            vmem((groups, cap, width), bf16),
            vmem((toks, toks), bf16),
            dma((9,)),
            dma((sends,)), dma((sends,)), dma((sends,)), dma((sends,)),
            dma((moves,)), dma((moves,)),
            dma((steps * groups,)), dma((steps * groups,)),
            dma((steps * (groups - 1),)), dma((steps * (groups - 1),)),
        ],
        compiler_params=pltpu.CompilerParams(
            collective_id=1, has_side_effects=True, vmem_limit_bytes=56 << 20
        ),
        cost_estimate=pl.CostEstimate(
            flops=12 * groups * cap * 2 * width * hidden, bytes_accessed=sent, transcendentals=0
        ),
    )(
        norm_gain[None, :], expert_group[None, :], expert_fine.T, route_weight.T,
        tokens, gate_master, up_master, down_master,
    )


def step(*args):
    tp_size = lax.axis_size("tp")
    gate_master = args[5]
    groups = gate_master.shape[0] // FINE
    if lax.axis_size("fs") == gate_master.shape[0] and tp_size > 2 and groups > 1 and gate_master.shape[2] % 128 == 0:
        return fused(*args)
    return local(*args)


def solution(mesh):
    in_specs = (
        P(("fs", "tp"), None),
        P(("fs", "tp")),
        P(("fs", "tp"), None),
        P(("fs", "tp"), None),
        P("fs"),
        P(None, "fs", "tp"),
        P(None, "fs", "tp"),
        P(None, "fs", "tp"),
    )
    out_specs = (
        P(("fs", "tp"), None),
        P("fs", None, None),
        P("fs", None, None),
        P("fs", None, None),
    )
    return jax.shard_map(step, mesh=mesh, in_specs=in_specs, out_specs=out_specs, check_vma=False)
```

```python
import functools

import jax
import jax.numpy as jnp
from jax import lax
from jax.experimental import pallas as pl
from jax.experimental.pallas import tpu as pltpu
from jax.sharding import PartitionSpec as P

FINE = 4


EPS = 1e-06


def flip(value, axis, bit):
    size = lax.axis_size(axis)
    return lax.ppermute(value, axis, [(i, i ^ bit) for i in range(size)])


def shift(value, axis, step):
    size = lax.axis_size(axis)
    return lax.ppermute(value, axis, [(i, (i + step) % size) for i in range(size)])


def gather_kernel(
    fs_size, tp_size, members, cap, tok_ref, piece_ref, x_ref, ready_ref,
    local_sem, tsend, trecv, psend, precv, xsend, xrecv, csend, crecv,
):
    groups, chips = fs_size // members, tp_size // 2
    tok_rows = tok_ref.shape[0]
    rows = piece_ref.shape[2]
    fs, tp = lax.axis_index("fs"), lax.axis_index("tp")
    group, member = fs // members, fs % members
    chip, core = tp // 2, tp % 2

    def away(r, i):
        base = member + i - 2 * (member & i)
        ahead = ((group + r) % groups) * members + base
        behind = ((group + groups - r) % groups) * members + base
        return ahead, behind

    def chip_tp(q, c):
        return ((chip + q) % chips) * 2 + c

    peers = [
        (away(r, i)[0], tp) for r in range(groups) for i in range(members) if r or i
    ]
    peers += [(fs, chip_tp(q, core)) for q in range(1, chips)] + [(fs, chip_tp(0, 1 - core))]
    barrier = pltpu.get_barrier_semaphore()
    for f, t in peers:
        pl.semaphore_signal(
            barrier, inc=1, device_id={"fs": f, "tp": t}, device_id_type=pl.DeviceIdType.MESH
        )
    pl.semaphore_wait(barrier, len(peers))

    started = []

    def send(src, dst, send_sem, recv_sem, f, t):
        copy = pltpu.make_async_remote_copy(
            src_ref=src, dst_ref=dst, send_sem=send_sem, recv_sem=recv_sem,
            device_id={"fs": f, "tp": t}, device_id_type=pl.DeviceIdType.MESH,
        )
        copy.start()
        started.append(copy)
        return copy

    near, far = pl.ds(0, cap), pl.ds(cap, tok_rows - cap)

    def pass_on(src, part, j, bit, k):
        return send(
            src, x_ref.at[j, part], tsend.at[k], trecv.at[k], away(0, bit)[0], tp
        )

    def block(f):
        return pl.ds(pl.multiple_of(f * rows, rows), rows)

    near_2 = pass_on(tok_ref.at[near], near, 2, 2, 0)
    near_1 = pass_on(tok_ref.at[near], near, 1, 1, 1)
    crossing = []
    for r in range(1, groups):
        part = pl.ds(r * cap, cap)
        crossing.append(
            send(tok_ref.at[part], x_ref.at[0, part], tsend.at[5 + r], trecv.at[5 + r], away(r, 0)[0], tp)
        )
    kept = pltpu.make_async_copy(tok_ref.at[near], x_ref.at[0, near], local_sem.at[0])
    kept.start()
    own = pltpu.make_async_copy(piece_ref.at[fs], ready_ref.at[tp, :, block(fs)], local_sem.at[1])
    own.start()

    pieces = {}
    for r in range(groups):
        for i in range(members):
            if r or i:
                k = r * members + i
                to = away(r, i)[0]
                pieces[r, i] = send(
                    piece_ref.at[to], ready_ref.at[tp, :, block(fs)], psend.at[k], precv.at[k], to, tp
                )
    own.wait()
    across = {}

    def cross_chips(r, i):
        here = ready_ref.at[tp, :, block(away(r, i)[1])]
        for q in range(1, chips):
            k = r * members + i
            across[q, r, i] = send(
                here, here, xsend.at[q - 1, k], xrecv.at[q - 1, k], fs, chip_tp(q, core)
            )

    beside = []

    def cross_cores(q, r):
        size = members * rows
        start = ((group + groups - r) % groups) * size
        here = ready_ref.at[chip_tp(chips - q, core), :, pl.ds(pl.multiple_of(start, size), size)]
        beside.append(
            send(here, here, csend.at[q, r], crecv.at[q, r], fs, chip_tp(0, 1 - core))
        )

    cross_chips(0, 0)
    for i in range(1, members):
        pieces[0, i].wait_recv()
        cross_chips(0, i)
    cross_cores(0, 0)
    near_2.wait_recv()
    near_3 = pass_on(x_ref.at[2, near], near, 3, 1, 2)
    for copy in crossing:
        copy.wait_recv()
    far_2 = pass_on(x_ref.at[0, far], far, 2, 2, 3)
    far_1 = pass_on(x_ref.at[0, far], far, 1, 1, 4)
    passed = False
    for r in range(1, groups):
        for i in range(members):
            pieces[r, i].wait_recv()
            cross_chips(r, i)
            if not passed and i == members // 2 - 1:
                passed = True
                far_2.wait_recv()
                far_3 = pass_on(x_ref.at[2, far], far, 3, 1, 5)
        cross_cores(0, r)
    for r in range(groups):
        for q in range(1, chips):
            for i in range(members):
                across[q, r, i].wait_recv()
            cross_cores(q, r)
    near_1.wait_recv()
    near_3.wait_recv()
    far_1.wait_recv()
    far_3.wait_recv()
    for copy in beside:
        copy.wait_recv()
    kept.wait()
    for copy in started:
        copy.wait_send()


def gather(ordered, pieces, members, cap):
    fs_size, tp_size = lax.axis_size("fs"), lax.axis_size("tp")
    experts_all, kinds, rows, cols = pieces.shape
    chips = tp_size // 2
    moves, crossings = 6, fs_size // members - 1
    dma = pltpu.SemaphoreType.DMA
    sent = 5 * ordered.size + 3 * pieces.size
    return pl.pallas_call(
        functools.partial(gather_kernel, fs_size, tp_size, members, cap),
        out_shape=(
            jax.ShapeDtypeStruct((members,) + ordered.shape, ordered.dtype),
            jax.ShapeDtypeStruct((tp_size, kinds, fs_size * rows, cols), pieces.dtype),
        ),
        in_specs=[pl.BlockSpec(memory_space=pltpu.VMEM)] * 2,
        out_specs=(pl.BlockSpec(memory_space=pl.ANY),) * 2,
        scratch_shapes=[
            dma((2,)),
            dma((moves + crossings,)),
            dma((moves + crossings,)),
            dma((fs_size,)),
            dma((fs_size,)),
            dma((max(chips - 1, 1), fs_size)),
            dma((max(chips - 1, 1), fs_size)),
            dma((chips, fs_size // members)),
            dma((chips, fs_size // members)),
        ],
        compiler_params=pltpu.CompilerParams(collective_id=0, has_side_effects=True),
        cost_estimate=pl.CostEstimate(flops=0, bytes_accessed=4 * sent, transcendentals=0),
    )(ordered, pieces)


def apply_rows(x_ref, mine_ref, gate_ref, up_ref, down_ref, kept_ref, sent_ref, kept_at, sent_at):
    members, cap, _ = x_ref.shape
    width, _ = gate_ref.shape
    x = x_ref[:, :, :width].reshape(members * cap, width)
    parts = x_ref[:, :, width:].reshape(members * cap, -1).astype(jnp.float32)
    weight = jnp.sum(parts * mine_ref[...], axis=1, keepdims=True)
    gate_value = jnp.dot(x, gate_ref[...], preferred_element_type=jnp.float32)
    upward = jnp.dot(x, up_ref[...], preferred_element_type=jnp.float32)
    activation = (gate_value / (1.0 + jnp.exp(-gate_value)) * upward).astype(jnp.bfloat16)
    step = min(width, 512)
    for at in range(0, width, step):
        out = lax.dot_general(
            activation,
            down_ref[at : at + step, :],
            (((1,), (1,)), ((), ())),
            preferred_element_type=jnp.float32,
        )
        out = (weight * out).astype(jnp.bfloat16)
        for ref, places in ((kept_ref, kept_at), (sent_ref, sent_at)):
            for i, j in enumerate(places):
                ref[i, :, at : at + step] = out[j * cap : (j + 1) * cap]


def first_kernel(kept_at, sent_at, x_ref, mine_ref, ready_ref, kept_ref, sent_ref, *whole_refs):
    @pl.when(pl.program_id(0) == 0)
    def _():
        cols = ready_ref.shape[3]
        for kind, ref in enumerate(whole_refs):
            for t in range(ready_ref.shape[0]):
                ref[0, :, t * cols : (t + 1) * cols] = ready_ref[t, kind]

    apply_rows(
        x_ref, mine_ref, *(ref.at[0] for ref in whole_refs), kept_ref, sent_ref, kept_at, sent_at
    )


def second_kernel(kept_at, sent_at, x_ref, mine_ref, gate_ref, up_ref, down_ref, kept_ref, sent_ref):
    apply_rows(
        x_ref, mine_ref, gate_ref.at[0], up_ref.at[0], down_ref.at[0],
        kept_ref, sent_ref, kept_at, sent_at,
    )


def expert_rows(x_all, mine, weights, cap, first_block, blocks, kept_at, sent_at):
    members, _, extended = x_all.shape
    gathered = len(weights) == 1
    if gathered:
        tp_size, kinds, width, cols = weights[0].shape
        whole = (1, width, tp_size * cols)
    else:
        whole = weights[0].shape
        width = whole[1]

    def fixed(shape):
        return pl.BlockSpec(shape, lambda i: (0,) * len(shape))

    half = jax.ShapeDtypeStruct((members // 2, blocks * cap, width), jnp.bfloat16)
    half_spec = pl.BlockSpec((members // 2, cap, width), lambda i: (0, i, 0))
    extra = 3 if gathered else 0
    body = functools.partial(first_kernel if gathered else second_kernel, kept_at, sent_at)
    hidden = whole[2]
    return pl.pallas_call(
        body,
        grid=(blocks,),
        in_specs=[
            pl.BlockSpec((members, cap, extended), lambda i: (0, i + first_block, 0)),
            fixed(mine.shape),
        ]
        + [fixed(w.shape) for w in weights],
        out_specs=[half_spec] * 2 + [fixed(whole)] * extra,
        out_shape=[half] * 2 + [jax.ShapeDtypeStruct(whole, jnp.bfloat16)] * extra,
        compiler_params=pltpu.CompilerParams(vmem_limit_bytes=56 << 20),
        cost_estimate=pl.CostEstimate(
            flops=6 * members * blocks * cap * width * hidden,
            bytes_accessed=2 * (6 * width * hidden + 2 * members * blocks * cap * width),
            transcendentals=members * blocks * cap * hidden,
        ),
    )(x_all, mine, *weights)


def local(
    tokens, expert_group, expert_fine, route_weight, norm_gain, gate_master, up_master, down_master
):
    tok_rows, width = tokens.shape
    fs_size = lax.axis_size("fs")
    experts_all = gate_master.shape[0]
    groups = experts_all // FINE
    members = fs_size // groups
    cap = tok_rows // groups
    fs_me = lax.axis_index("fs")
    group_me, fine_me = fs_me // members, fs_me % members

    widened = tokens.astype(jnp.float32)
    normed = (
        widened * lax.rsqrt(jnp.mean(widened * widened, axis=-1, keepdims=True) + EPS)
    ).astype(jnp.bfloat16)
    away = (expert_group - group_me + groups) % groups
    index = jnp.arange(tok_rows, dtype=jnp.int32)
    same = (away[:, None] == away[None, :]) & (index[None, :] < index[:, None])
    slot = away * cap + jnp.sum(same.astype(jnp.int32), axis=1)
    placing = (index[:, None] == slot[None, :]).astype(jnp.bfloat16)
    fines = jnp.arange(FINE, dtype=jnp.int32)
    share = jnp.sum(
        jnp.where(expert_fine[:, None, :] == fines[None, :, None], route_weight[:, None, :], 0.0),
        axis=2,
    )
    high = lax.reduce_precision(share, 8, 7)
    middle = lax.reduce_precision(share - high, 8, 7)
    low = share - high - middle
    terms = jnp.concatenate([high, middle, low], axis=1).astype(jnp.bfloat16)
    terms = jnp.pad(terms, ((0, 0), (0, 128 - terms.shape[1])))
    extended = jnp.concatenate([normed, terms], axis=1)
    ordered = jnp.dot(placing, extended, preferred_element_type=jnp.float32).astype(jnp.bfloat16)

    pieces = jnp.stack(
        [norm_gain[None, :, None] * gate_master, norm_gain[None, :, None] * up_master, down_master],
        axis=1,
    ).astype(jnp.bfloat16)
    x_all, ready = gather(ordered, pieces, members, cap)
    lanes = jnp.arange(128, dtype=jnp.int32)
    mine = ((lanes % FINE == fine_me) & (lanes < 3 * FINE)).astype(jnp.float32)[None, :]

    def collect(kept, sent, first, second):
        far_part = flip(sent, "fs", second)
        pair = (kept.astype(jnp.float32) + far_part.astype(jnp.float32)).astype(jnp.bfloat16)
        back = flip(pair[1], "fs", first)
        return (pair[0].astype(jnp.float32) + back.astype(jnp.float32)).astype(jnp.bfloat16)

    kept, sent, gate_ready, up_ready, down_ready = expert_rows(
        x_all, mine, (ready,), cap, 1, groups - 1, (0, 2), (1, 3)
    )
    far_mixed = collect(kept, sent, 2, 1)
    kept, sent = expert_rows(
        x_all, mine, (gate_ready, up_ready, down_ready), cap, 0, 1, (0, 1), (2, 3)
    )
    near_mixed = collect(kept, sent, 1, 2)
    returned = [near_mixed] + [
        shift(far_mixed[(r - 1) * cap : r * cap], "fs", -r * members) for r in range(1, groups)
    ]
    mixed = lax.dot_general(
        placing,
        jnp.concatenate(returned),
        (((0,), (0,)), ((), ())),
        preferred_element_type=jnp.float32,
    ).astype(jnp.bfloat16)
    return (mixed, gate_ready, up_ready, down_ready)


def fused_kernel(
    groups, chips, cap, gain_ref, group_ref, fine_ref, weight_ref, tok_hbm, gate_hbm, up_hbm, down_hbm,
    place_out, ret_out, gate_out, up_out, down_out,
    master, tok, piece_gu, piece_dn, w_gu, w_dn, x_rows, far_rows, share, far_share, act,
    y_send, y_recv, part, z_send, ret, place,
    lsem, gsend, grecv, dsend, drecv, tsend, trecv, ysend, yrecv, zsend, zrecv,
):
    rows, cols = piece_gu.shape[4:]
    toks, width = tok.shape
    hidden = w_dn.shape[2]
    fs, tp = lax.axis_index("fs"), lax.axis_index("tp")
    group, bit, side = fs // FINE, (fs // 2) % 2, fs % 2
    chip, core = tp // 2, tp % 2
    bf16, f32 = jnp.bfloat16, jnp.float32

    def ahead(r):
        return (group + r) % groups

    def behind(r):
        return (group + groups - r) % groups

    def member(grp, bb, jj):
        return grp * FINE + (bit + bb - 2 * bit * bb) * 2 + (side + jj - 2 * side * jj)

    def flipped(a, b):
        return a + b - 2 * a * b

    def entry(grp):
        return 1 - grp % 2

    def source(r, bb, jj):
        grp = behind(r)
        if r == 0:
            return member(grp, bb, jj)
        return grp * FINE + flipped(entry(grp), bb) * 2 + flipped(side, jj)

    def chip_ahead(q):
        return (chip + q) % chips

    def chip_behind(q):
        return (chip + chips - q) % chips

    def block(f):
        return pl.ds(pl.multiple_of(f * rows, rows), rows)

    def lanes(t):
        return pl.ds(pl.multiple_of(t * cols, cols), cols)

    loads = []
    for k, (src, dst) in enumerate(
        ((gate_hbm, master.at[0]), (up_hbm, master.at[1]), (tok_hbm, tok), (down_hbm, master.at[2]))
    ):
        copy = pltpu.make_async_copy(src, dst, lsem.at[k])
        copy.start()
        loads.append(copy)

    links = [(member(group, 0, 1), tp), (member(group, 1, 0), tp)]
    links += [(ahead(r) * FINE + m, tp) for r in range(1, groups) for m in range(FINE)]
    links += [(fs, chip_ahead(q) * 2 + core) for q in range(1, chips)] + [(fs, chip * 2 + 1 - core)]
    barrier = pltpu.get_barrier_semaphore()
    for f, t in links:
        pl.semaphore_signal(
            barrier, inc=1, device_id={"fs": f, "tp": t}, device_id_type=pl.DeviceIdType.MESH
        )

    inner = bit == entry(group)
    outer = jnp.logical_not(inner)

    def remote(src, dst, send_sem, recv_sem, f, t):
        return pltpu.make_async_remote_copy(
            src_ref=src, dst_ref=dst, send_sem=send_sem, recv_sem=recv_sem,
            device_id={"fs": f, "tp": t}, device_id_type=pl.DeviceIdType.MESH,
        )

    gain = jnp.transpose(jnp.broadcast_to(gain_ref[...], (cols, rows)))
    loads[0].wait()
    loads[1].wait()
    experts_all = master.shape[1]
    for e in range(experts_all):
        for kind in (0, 1):
            piece_gu[e // FINE, e % 2, (e % FINE) // 2, kind] = (gain * master[kind, e]).astype(bf16)
    pl.semaphore_wait(barrier, len(links))

    count = 4 * groups
    keys = [(r, bb, jj) for r in range(groups) for bb in (0, 1) for jj in (0, 1)]

    class Route:
        def __init__(self, piece, whole, send_sem, recv_sem):
            self.piece, self.whole, self.lead = piece, whole, (slice(None),) * (len(whole.shape) - 2)
            self.send_sem, self.recv_sem = send_sem, recv_sem

        def region(self, f, t):
            return self.whole.at[self.lead + (block(f), lanes(t))]

        def move(self, src, dst, sent, received, f, t):
            return remote(src, dst, self.send_sem.at[sent], self.recv_sem.at[received], f, t)

        def src(self, key):
            return self.region(source(*key), tp) if any(key) else self.piece.at[group, side]

        def land(self, key):
            r, bb, jj = key
            k = keys.index(key)
            if key == (0, 0, 1):
                piece = self.piece.at[group, flipped(side, 1)]
                return self.move(piece, self.region(fs, tp), k, k, member(group, 0, 1), tp)
            first = key if r else (0, 0, jj)
            here = self.region(source(*first), tp)
            return self.move(self.src(first), here, k, k, member(group, 1, 0), tp)

        def direct(self, r, jj):
            j = flipped(side, jj)
            to = ahead(r) * FINE + entry(ahead(r)) * 2 + j
            slot = r * 4 + flipped(bit, entry(group)) * 2 + jj
            piece = self.piece.at[ahead(r), j]
            return self.move(piece, self.region(fs, tp), count + r * 2 + jj, slot, to, tp)

        def across(self, key, q):
            here = self.region(source(*key), tp)
            k = count + keys.index(key) * (chips - 1) + q - 1
            return self.move(self.src(key), here, k + 2 * groups, k, fs, chip_ahead(q) * 2 + core)

        def beside(self, key, q):
            here = self.region(source(*key), chip_behind(q) * 2 + core)
            src = self.src(key) if q == 0 else here
            k = count * chips + keys.index(key) * chips + q
            return self.move(src, here, k + 2 * groups, k, fs, chip * 2 + 1 - core)

        def hand(self, key):
            for q in range(1, chips):
                self.across(key, q).start()
            self.beside(key, 0).start()

        def arrived(self, key, forward=False):
            self.land(key).wait_recv()
            if forward:
                self.land(key).start()
            if key == (0, 0, 1):
                self.land((0, 1, 1)).start()
            self.hand(key)

        def crossed(self, key):
            for q in range(1, chips):
                self.across(key, q).wait_recv()
                self.beside(key, q).start()

        def directs(self):
            for r in range(1, groups):
                for jj in (0, 1):
                    self.direct(r, jj).start()

        def drain(self):
            for key in keys:
                if any(key) and not key[0]:
                    self.land(key).wait_send()
                for q in range(chips):
                    if q:
                        self.across(key, q).wait_send()
                    self.beside(key, q).wait_send()
            for r in range(1, groups):
                for jj in (0, 1):
                    self.direct(r, jj).wait_send()

            @pl.when(inner)
            def _():
                for key in keys[4:]:
                    self.land(key).wait_send()

    gu = Route(piece_gu, w_gu, gsend, grecv)
    dn = Route(piece_dn, w_dn, dsend, drecv)

    gu.land((0, 0, 1)).start()
    gu.land((0, 1, 0)).start()
    gu.hand((0, 0, 0))
    pl.when(inner)(gu.directs)
    keep_gu = pltpu.make_async_copy(piece_gu.at[group, side], gu.region(fs, tp), lsem.at[4])
    keep_gu.start()

    loads[2].wait()
    pad = max(8, groups)
    away = group_ref[...] - group
    away = jnp.where(away < 0, away + groups, away)
    which = lax.broadcasted_iota(jnp.int32, (pad, toks), 0)
    mine = (which == away).astype(f32)
    first = lax.broadcasted_iota(jnp.int32, (toks, toks), 0)
    second = lax.broadcasted_iota(jnp.int32, (toks, toks), 1)
    before = jnp.dot(
        mine.astype(bf16), (first < second).astype(f32).astype(bf16), preferred_element_type=f32
    )
    slot = jnp.sum(mine * (before + (which * cap).astype(f32)), axis=0, keepdims=True)
    placing = (first.astype(f32) == slot).astype(f32)
    place[...] = placing.astype(bf16)
    finer = lax.broadcasted_iota(jnp.int32, (8, toks), 0)
    shares = jnp.zeros((8, toks), f32)
    for k in range(fine_ref.shape[0]):
        shares += jnp.where(finer == fine_ref[k : k + 1, :], weight_ref[k : k + 1, :], 0.0)
    shares = lax.dot_general(
        shares, placing, (((1,), (1,)), ((), ())),
        preferred_element_type=f32, precision=lax.Precision.HIGHEST,
    )

    def normed(r):
        raw = jnp.dot(place[r * cap : (r + 1) * cap, :], tok[...], preferred_element_type=f32)
        scale = lax.rsqrt(jnp.mean(raw * raw, axis=1, keepdims=True) + EPS)
        return (raw * scale).astype(bf16)

    def at(r, jj):
        return pl.ds((r * 2 + jj) * cap, cap)

    share[0, 0] = shares[:, :cap]
    for r in range(1, groups):
        far_share[r - 1] = shares[:, r * cap : (r + 1) * cap]
    x_rows[at(0, 0), :] = normed(0)
    mate = member(group, 0, 1)
    parts = 2
    step = cap // parts

    def rows_move(k, src, dst, f):
        return remote(src, dst, tsend.at[k], trecv.at[k], f, tp)

    def near():
        return [
            rows_move(0, share.at[0, 0], share.at[0, 1], mate),
            rows_move(1, x_rows.at[at(0, 0)], x_rows.at[at(0, 1)], mate),
        ]

    def far(r):
        to, base = member(ahead(r), 0, 0), 2 + (r - 1) * 2 * (parts + 1)
        moves = [rows_move(base, far_share.at[r - 1], share.at[r, 0], to)]
        for p in range(parts):
            here = pl.ds(r * 2 * cap + p * step, step)
            src = far_rows.at[r - 1, pl.ds(p * step, step)]
            moves.append(rows_move(base + 1 + p, src, x_rows.at[here], to))
        return moves

    def passed(r):
        base = 2 + (r - 1) * 2 * (parts + 1) + parts + 1
        moves = [rows_move(base, share.at[r, 0], share.at[r, 1], mate)]
        for p in range(parts):
            here = pl.ds(r * 2 * cap + p * step, step)
            there = pl.ds((r * 2 + 1) * cap + p * step, step)
            moves.append(rows_move(base + 1 + p, x_rows.at[here], x_rows.at[there], mate))
        return moves

    def start_far():
        for r in range(1, groups):
            for move in far(r):
                move.start()

    def pass_far():
        for r in range(1, groups):
            for landed, move in zip(far(r), passed(r)):
                landed.wait_recv()
                move.start()

    for move in near():
        move.start()
    for r in range(1, groups):
        far_rows[r - 1] = normed(r)

    loads[3].wait()
    for e in range(experts_all):
        piece_dn[e // FINE, e % 2, (e % FINE) // 2] = master[2, e].astype(bf16)
    keep_dn = pltpu.make_async_copy(piece_dn.at[group, side], dn.region(fs, tp), lsem.at[5])
    keep_dn.start()
    others = range(1, groups)
    inner_order = [(0, 0, 0), (0, 1, 0), (0, 0, 1)]
    inner_order += [(r, 0, jj) for r in others for jj in (0, 1)] + [(0, 1, 1)]
    inner_order += [(r, 1, jj) for r in others for jj in (0, 1)]
    outer_order = [(0, 0, 0), (0, 0, 1), (0, 1, 0), (0, 1, 1)]
    outer_order += [(r, bb, jj) for r in others for bb in (0, 1) for jj in (0, 1)]
    ahead_of = 3

    def route_gates(order, forward):
        done = 0
        for k, key in enumerate(order[1:]):
            gu.arrived(key, forward and key[0] > 0)
            if key == (0, 0, 1):
                dn.land((0, 0, 1)).start()
                dn.beside((0, 0, 0), 0).start()
                if not forward:
                    gu.directs()
                    start_far()
            if k >= ahead_of:
                gu.crossed(order[done])
                done += 1
        if forward:
            start_far()
        for q in range(1, chips):
            dn.across((0, 0, 0), q).start()

    pl.when(inner)(lambda: route_gates(inner_order, True))
    pl.when(outer)(lambda: route_gates(outer_order, False))

    def apply_rows(start, count, s, lane0, lane_count):
        here = pl.ds(start * cap, count * cap)
        x = x_rows[here, :]
        at_lanes = pl.ds(pl.multiple_of(lane0, cols), lane_count)
        gate_value = jnp.dot(x, w_gu[s, 0, :, at_lanes], preferred_element_type=f32)
        upward = jnp.dot(x, w_gu[s, 1, :, at_lanes], preferred_element_type=f32)
        fine = s * 2 + side
        chosen = []
        for i in range(start, start + count):
            flat = jnp.transpose(share[i // 2, i % 2])
            lane = lax.broadcasted_iota(jnp.int32, flat.shape, 1)
            chosen.append(jnp.sum(jnp.where(lane == fine, flat, 0.0), axis=1, keepdims=True))
        weight = jnp.concatenate(chosen, axis=0)
        value = gate_value / (1.0 + jnp.exp(-gate_value)) * upward * weight
        act[here, pl.ds(pl.multiple_of(s * hidden + lane0, cols), lane_count)] = value.astype(bf16)

    keep_gu.wait()
    for key in keys:
        if any(key):
            gu.beside(key, 0).wait_recv()
    gu.beside((0, 0, 0), 0).wait_recv()
    for move in near():
        move.wait_recv()
    pair = 2 * cols
    for s in (0, 1):
        apply_rows(0, 2, s, chip * pair, pair)

    def finish_gates(order, forward):
        rest = order[len(order) - 1 - ahead_of :]
        dn.land((0, 0, 1)).wait_recv()
        dn.hand((0, 0, 1))
        if not forward:
            dn.land((0, 1, 0)).start()
            dn.land((0, 1, 1)).start()
        for k, key in enumerate(rest):
            if k == len(rest) - (2 if forward else 1):
                pass_far()
            if k == len(rest) - (0 if forward else 1):
                if forward:
                    dn.land((0, 1, 0)).start()
                    dn.land((0, 1, 1)).start()
                dn.directs()
            gu.crossed(key)
        if forward:
            dn.land((0, 1, 0)).start()
            dn.land((0, 1, 1)).start()
            dn.directs()

    pl.when(inner)(lambda: finish_gates(inner_order, True))
    pl.when(outer)(lambda: finish_gates(outer_order, False))
    for key in keys:
        for q in range(1, chips):
            gu.beside(key, q).wait_recv()
    for q in range(1, chips):
        for s in (0, 1):
            apply_rows(0, 2, s, chip_behind(q) * pair, pair)
    outs = [
        pltpu.make_async_copy(w_gu.at[bit, 0], gate_out.at[0], lsem.at[6]),
        pltpu.make_async_copy(w_gu.at[bit, 1], up_out.at[0], lsem.at[7]),
    ]
    for copy in outs:
        copy.start()

    keep_dn.wait()
    span = 2 * rows
    steps = [(r, bb) for r in range(groups) for bb in (0, 1)]

    def columns(n, cut, cuts, base=group):
        r, bb = steps[n]
        wide = span // cuts
        grp = (base + groups - r) % groups
        pick = flipped(entry(grp) if r else bit, bb)
        start = (grp * FINE + pick * 2) * rows + cut * wide
        return pl.ds(pl.multiple_of(start, wide), wide)

    crossing, home = {}, {}

    def ready(n):
        r, bb = steps[n]
        for jj in (0, 1):
            dn.crossed((r, bb, jj))
        for jj in (0, 1):
            for q in range(chips):
                dn.beside((r, bb, jj), q).wait_recv()

    def produce(n, r, cut, cuts):
        here = columns(n, cut, cuts)
        mine = pl.ds(r * 2 * cap, 2 * cap)
        out = jnp.zeros((2 * cap, span // cuts), f32)
        for s in (0, 1):
            out += lax.dot_general(
                act[mine, s * hidden : (s + 1) * hidden], w_dn[s, here, :],
                (((1,), (1,)), ((), ())), preferred_element_type=f32,
            )
        y_send[r, :, here] = out[cap:].astype(bf16)
        part[r, :, here] = out[:cap]
        k = len(crossing)
        crossing[n, r, cut, cuts] = remote(
            y_send.at[r, :, here], y_recv.at[r, :, here], ysend.at[k], yrecv.at[k], mate, tp
        )
        crossing[n, r, cut, cuts].start()
        waiting.append((n, r, cut, cuts))

    def combine(n, r, cut, cuts):
        here = columns(n, cut, cuts)
        crossing[n, r, cut, cuts].wait_recv()
        total = (part[r, :, here] + y_recv[r, :, here].astype(f32)).astype(bf16)
        if r == 0:
            ret[0, :, here] = total
        else:
            z_send[r - 1, :, here] = total
            k = len(home)
            home[n, r, cut] = remote(
                z_send.at[r - 1, :, here], ret.at[r, :, here], zsend.at[k], zrecv.at[k],
                member(behind(r), 0, 0), tp,
            )
            home[n, r, cut].start()

    waiting = []

    def far_down(bb):
        for r in others:
            for jj in (0, 1):
                dn.arrived((r, bb, jj), True)

    def far_down_outer(bb):
        for r in others:
            for jj in (0, 1):
                dn.arrived((r, bb, jj))

    def near_down():
        dn.arrived((0, 1, 0))
        dn.arrived((0, 1, 1))

    pl.when(outer)(near_down)
    for r in others:
        for move in passed(r):
            move.wait_recv()
        for s in (0, 1):
            for half in range(chips):
                apply_rows(2 * r, 2, s, half * pair, pair)
    pl.when(inner)(near_down)
    ready(0)
    for r in reversed(range(groups)):
        produce(0, r, 0, 1)
    pl.when(inner)(lambda: far_down(0))
    pl.when(outer)(lambda: far_down_outer(0))
    pl.when(inner)(lambda: far_down(1))
    last = len(steps) - 1
    for n in range(1, len(steps)):
        if n == 2:
            pl.when(outer)(lambda: far_down_outer(1))
        ready(n)
        cuts = 2 if n == last else 1
        for r in reversed(range(groups)):
            for cut in range(cuts):
                produce(n, r, cut, cuts)
                if len(waiting) > groups:
                    combine(*waiting.pop(0))
    outs.append(pltpu.make_async_copy(w_dn.at[bit], down_out.at[0], lsem.at[8]))
    outs[-1].start()
    outs.append(pltpu.make_async_copy(place, place_out, lsem.at[10]))
    outs[-1].start()
    for item in waiting:
        combine(*item)
    outs.append(pltpu.make_async_copy(ret.at[0], ret_out.at[0], lsem.at[9]))
    outs[-1].start()
    gu.drain()
    dn.drain()
    for move in near():
        move.wait_send()
    for r in others:
        for move in far(r) + passed(r):
            move.wait_send()
    for k, ((n, r, cut), copy) in enumerate(home.items()):
        copy.wait_recv()
        here = columns(n, cut, 2 if n == last else 1, ahead(r))
        outs.append(
            pltpu.make_async_copy(ret.at[r, :, here], ret_out.at[r, :, here], lsem.at[11 + k])
        )
        outs[-1].start()
    for copy in list(crossing.values()) + list(home.values()):
        copy.wait_send()
    for copy in outs:
        copy.wait()


def publish_kernel(
    place_ref, ret_ref, gate_ref, up_ref, down_ref, mixed_out, gate_out, up_out, down_out,
    mixed, out_sem, row_sem,
):
    writes = [
        pltpu.make_async_copy(src, dst, out_sem.at[k])
        for k, (src, dst) in enumerate(
            ((gate_ref, gate_out), (up_ref, up_out), (down_ref, down_out))
        )
    ]
    for write in writes:
        write.start()
    width = ret_ref.shape[1]
    chunk = min(width, 512)
    for c in range(0, width, chunk):
        here = pl.ds(c, chunk)
        mixed[:, here] = lax.dot_general(
            place_ref[...], ret_ref[:, here], (((0,), (0,)), ((), ())),
            preferred_element_type=jnp.float32,
        ).astype(jnp.bfloat16)
    last = pltpu.make_async_copy(mixed, mixed_out, row_sem)
    last.start()
    last.wait()
    for write in writes:
        write.wait()


def publish(placed, returned, gate, up, down):
    toks, width = returned.shape
    anywhere = pl.BlockSpec(memory_space=pl.ANY)
    local_spec = pl.BlockSpec(memory_space=pltpu.VMEM)
    whole = jax.ShapeDtypeStruct(gate.shape, gate.dtype)
    return pl.pallas_call(
        publish_kernel,
        out_shape=(jax.ShapeDtypeStruct((toks, width), returned.dtype), whole, whole, whole),
        in_specs=[local_spec] * 2 + [anywhere] * 3,
        out_specs=(anywhere,) * 4,
        scratch_shapes=[
            pltpu.VMEM((toks, width), returned.dtype),
            pltpu.SemaphoreType.DMA((3,)),
            pltpu.SemaphoreType.DMA,
        ],
        compiler_params=pltpu.CompilerParams(vmem_limit_bytes=12 << 20),
        cost_estimate=pl.CostEstimate(
            flops=2 * toks * toks * width, bytes_accessed=6 * gate.size * 2, transcendentals=0
        ),
    )(placed, returned, gate, up, down)


def fused(
    tokens, expert_group, expert_fine, route_weight, norm_gain, gate_master, up_master, down_master
):
    toks, width = tokens.shape
    fs_size, tp_size = lax.axis_size("fs"), lax.axis_size("tp")
    experts_all, rows, cols = gate_master.shape
    groups, chips, hidden = experts_all // FINE, tp_size // 2, cols * tp_size
    cap = toks // groups
    bf16, f32 = jnp.bfloat16, jnp.float32
    sources = groups * 4
    sends = sources * 2 * chips + 2 * groups
    moves = 2 + (groups - 1) * 6
    steps = 2 * groups
    vmem, dma = pltpu.VMEM, pltpu.SemaphoreType.DMA
    anywhere = pl.BlockSpec(memory_space=pl.ANY)
    local_spec = pl.BlockSpec(memory_space=pltpu.VMEM)
    sent = 2 * (3 * width * hidden * 2 + 6 * toks * width)
    placed, returned, *ready = pl.pallas_call(
        functools.partial(fused_kernel, groups, chips, cap),
        out_shape=(
            vmem((toks, toks), bf16),
            vmem((groups, cap, width), bf16),
            vmem((1, width, hidden), bf16),
            vmem((1, width, hidden), bf16),
            vmem((1, width, hidden), bf16),
        ),
        in_specs=[local_spec] * 4 + [pl.BlockSpec(memory_space=pltpu.HBM)] * 4,
        out_specs=(anywhere,) * 5,
        scratch_shapes=[
            vmem((3, experts_all, rows, cols), f32),
            vmem((toks, width), bf16),
            vmem((groups, 2, 2, 2, rows, cols), bf16),
            vmem((groups, 2, 2, rows, cols), bf16),
            vmem((2, 2, width, hidden), bf16),
            vmem((2, width, hidden), bf16),
            vmem((2 * groups * cap, width), bf16),
            vmem((groups - 1, cap, width), bf16),
            vmem((groups, 2, 8, cap), f32),
            vmem((groups - 1, 8, cap), f32),
            vmem((2 * groups * cap, 2 * hidden), bf16),
            vmem((groups, cap, width), bf16),
            vmem((groups, cap, width), bf16),
            vmem((groups, cap, width), f32),
            vmem((groups - 1, cap, width), bf16),
            vmem((groups, cap, width), bf16),
            vmem((toks, toks), bf16),
            dma((11 + (steps + 1) * (groups - 1),)),
            dma((sends,)), dma((sends,)), dma((sends,)), dma((sends,)),
            dma((moves,)), dma((moves,)),
            dma(((steps + 1) * groups,)), dma(((steps + 1) * groups,)),
            dma(((steps + 1) * (groups - 1),)), dma(((steps + 1) * (groups - 1),)),
        ],
        compiler_params=pltpu.CompilerParams(
            collective_id=1, has_side_effects=True, vmem_limit_bytes=56 << 20
        ),
        cost_estimate=pl.CostEstimate(
            flops=12 * groups * cap * 2 * width * hidden, bytes_accessed=sent, transcendentals=0
        ),
    )(
        norm_gain[None, :], expert_group[None, :], expert_fine.T, route_weight.T,
        tokens, gate_master, up_master, down_master,
    )
    return publish(placed, returned.reshape(toks, width), *ready)


def step(*args):
    tp_size = lax.axis_size("tp")
    gate_master = args[5]
    groups = gate_master.shape[0] // FINE
    if lax.axis_size("fs") == gate_master.shape[0] and tp_size > 2 and groups > 1 and gate_master.shape[2] % 128 == 0:
        return fused(*args)
    return local(*args)


def solution(mesh):
    in_specs = (
        P(("fs", "tp"), None),
        P(("fs", "tp")),
        P(("fs", "tp"), None),
        P(("fs", "tp"), None),
        P("fs"),
        P(None, "fs", "tp"),
        P(None, "fs", "tp"),
        P(None, "fs", "tp"),
    )
    out_specs = (
        P(("fs", "tp"), None),
        P("fs", None, None),
        P("fs", None, None),
        P("fs", None, None),
    )
    return jax.shard_map(step, mesh=mesh, in_specs=in_specs, out_specs=out_specs, check_vma=False)
```

```python
import functools

import jax
import jax.numpy as jnp
from jax import lax
from jax.experimental import pallas as pl
from jax.experimental.pallas import tpu as pltpu
from jax.sharding import PartitionSpec as P

FINE = 4


EPS = 1e-06


def flip(value, axis, bit):
    size = lax.axis_size(axis)
    return lax.ppermute(value, axis, [(i, i ^ bit) for i in range(size)])


def shift(value, axis, step):
    size = lax.axis_size(axis)
    return lax.ppermute(value, axis, [(i, (i + step) % size) for i in range(size)])


def gather_kernel(
    fs_size, tp_size, members, cap, tok_ref, piece_ref, x_ref, ready_ref,
    local_sem, tsend, trecv, psend, precv, xsend, xrecv, csend, crecv,
):
    groups, chips = fs_size // members, tp_size // 2
    tok_rows = tok_ref.shape[0]
    rows = piece_ref.shape[2]
    fs, tp = lax.axis_index("fs"), lax.axis_index("tp")
    group, member = fs // members, fs % members
    chip, core = tp // 2, tp % 2

    def away(r, i):
        base = member + i - 2 * (member & i)
        ahead = ((group + r) % groups) * members + base
        behind = ((group + groups - r) % groups) * members + base
        return ahead, behind

    def chip_tp(q, c):
        return ((chip + q) % chips) * 2 + c

    peers = [
        (away(r, i)[0], tp) for r in range(groups) for i in range(members) if r or i
    ]
    peers += [(fs, chip_tp(q, core)) for q in range(1, chips)] + [(fs, chip_tp(0, 1 - core))]
    barrier = pltpu.get_barrier_semaphore()
    for f, t in peers:
        pl.semaphore_signal(
            barrier, inc=1, device_id={"fs": f, "tp": t}, device_id_type=pl.DeviceIdType.MESH
        )
    pl.semaphore_wait(barrier, len(peers))

    started = []

    def send(src, dst, send_sem, recv_sem, f, t):
        copy = pltpu.make_async_remote_copy(
            src_ref=src, dst_ref=dst, send_sem=send_sem, recv_sem=recv_sem,
            device_id={"fs": f, "tp": t}, device_id_type=pl.DeviceIdType.MESH,
        )
        copy.start()
        started.append(copy)
        return copy

    near, far = pl.ds(0, cap), pl.ds(cap, tok_rows - cap)

    def pass_on(src, part, j, bit, k):
        return send(
            src, x_ref.at[j, part], tsend.at[k], trecv.at[k], away(0, bit)[0], tp
        )

    def block(f):
        return pl.ds(pl.multiple_of(f * rows, rows), rows)

    near_2 = pass_on(tok_ref.at[near], near, 2, 2, 0)
    near_1 = pass_on(tok_ref.at[near], near, 1, 1, 1)
    crossing = []
    for r in range(1, groups):
        part = pl.ds(r * cap, cap)
        crossing.append(
            send(tok_ref.at[part], x_ref.at[0, part], tsend.at[5 + r], trecv.at[5 + r], away(r, 0)[0], tp)
        )
    kept = pltpu.make_async_copy(tok_ref.at[near], x_ref.at[0, near], local_sem.at[0])
    kept.start()
    own = pltpu.make_async_copy(piece_ref.at[fs], ready_ref.at[tp, :, block(fs)], local_sem.at[1])
    own.start()

    pieces = {}
    for r in range(groups):
        for i in range(members):
            if r or i:
                k = r * members + i
                to = away(r, i)[0]
                pieces[r, i] = send(
                    piece_ref.at[to], ready_ref.at[tp, :, block(fs)], psend.at[k], precv.at[k], to, tp
                )
    own.wait()
    across = {}

    def cross_chips(r, i):
        here = ready_ref.at[tp, :, block(away(r, i)[1])]
        for q in range(1, chips):
            k = r * members + i
            across[q, r, i] = send(
                here, here, xsend.at[q - 1, k], xrecv.at[q - 1, k], fs, chip_tp(q, core)
            )

    beside = []

    def cross_cores(q, r):
        size = members * rows
        start = ((group + groups - r) % groups) * size
        here = ready_ref.at[chip_tp(chips - q, core), :, pl.ds(pl.multiple_of(start, size), size)]
        beside.append(
            send(here, here, csend.at[q, r], crecv.at[q, r], fs, chip_tp(0, 1 - core))
        )

    cross_chips(0, 0)
    for i in range(1, members):
        pieces[0, i].wait_recv()
        cross_chips(0, i)
    cross_cores(0, 0)
    near_2.wait_recv()
    near_3 = pass_on(x_ref.at[2, near], near, 3, 1, 2)
    for copy in crossing:
        copy.wait_recv()
    far_2 = pass_on(x_ref.at[0, far], far, 2, 2, 3)
    far_1 = pass_on(x_ref.at[0, far], far, 1, 1, 4)
    passed = False
    for r in range(1, groups):
        for i in range(members):
            pieces[r, i].wait_recv()
            cross_chips(r, i)
            if not passed and i == members // 2 - 1:
                passed = True
                far_2.wait_recv()
                far_3 = pass_on(x_ref.at[2, far], far, 3, 1, 5)
        cross_cores(0, r)
    for r in range(groups):
        for q in range(1, chips):
            for i in range(members):
                across[q, r, i].wait_recv()
            cross_cores(q, r)
    near_1.wait_recv()
    near_3.wait_recv()
    far_1.wait_recv()
    far_3.wait_recv()
    for copy in beside:
        copy.wait_recv()
    kept.wait()
    for copy in started:
        copy.wait_send()


def gather(ordered, pieces, members, cap):
    fs_size, tp_size = lax.axis_size("fs"), lax.axis_size("tp")
    experts_all, kinds, rows, cols = pieces.shape
    chips = tp_size // 2
    moves, crossings = 6, fs_size // members - 1
    dma = pltpu.SemaphoreType.DMA
    sent = 5 * ordered.size + 3 * pieces.size
    return pl.pallas_call(
        functools.partial(gather_kernel, fs_size, tp_size, members, cap),
        out_shape=(
            jax.ShapeDtypeStruct((members,) + ordered.shape, ordered.dtype),
            jax.ShapeDtypeStruct((tp_size, kinds, fs_size * rows, cols), pieces.dtype),
        ),
        in_specs=[pl.BlockSpec(memory_space=pltpu.VMEM)] * 2,
        out_specs=(pl.BlockSpec(memory_space=pl.ANY),) * 2,
        scratch_shapes=[
            dma((2,)),
            dma((moves + crossings,)),
            dma((moves + crossings,)),
            dma((fs_size,)),
            dma((fs_size,)),
            dma((max(chips - 1, 1), fs_size)),
            dma((max(chips - 1, 1), fs_size)),
            dma((chips, fs_size // members)),
            dma((chips, fs_size // members)),
        ],
        compiler_params=pltpu.CompilerParams(collective_id=0, has_side_effects=True),
        cost_estimate=pl.CostEstimate(flops=0, bytes_accessed=4 * sent, transcendentals=0),
    )(ordered, pieces)


def apply_rows(x_ref, mine_ref, gate_ref, up_ref, down_ref, kept_ref, sent_ref, kept_at, sent_at):
    members, cap, _ = x_ref.shape
    width, _ = gate_ref.shape
    x = x_ref[:, :, :width].reshape(members * cap, width)
    parts = x_ref[:, :, width:].reshape(members * cap, -1).astype(jnp.float32)
    weight = jnp.sum(parts * mine_ref[...], axis=1, keepdims=True)
    gate_value = jnp.dot(x, gate_ref[...], preferred_element_type=jnp.float32)
    upward = jnp.dot(x, up_ref[...], preferred_element_type=jnp.float32)
    activation = (gate_value / (1.0 + jnp.exp(-gate_value)) * upward).astype(jnp.bfloat16)
    step = min(width, 512)
    for at in range(0, width, step):
        out = lax.dot_general(
            activation,
            down_ref[at : at + step, :],
            (((1,), (1,)), ((), ())),
            preferred_element_type=jnp.float32,
        )
        out = (weight * out).astype(jnp.bfloat16)
        for ref, places in ((kept_ref, kept_at), (sent_ref, sent_at)):
            for i, j in enumerate(places):
                ref[i, :, at : at + step] = out[j * cap : (j + 1) * cap]


def first_kernel(kept_at, sent_at, x_ref, mine_ref, ready_ref, kept_ref, sent_ref, *whole_refs):
    @pl.when(pl.program_id(0) == 0)
    def _():
        cols = ready_ref.shape[3]
        for kind, ref in enumerate(whole_refs):
            for t in range(ready_ref.shape[0]):
                ref[0, :, t * cols : (t + 1) * cols] = ready_ref[t, kind]

    apply_rows(
        x_ref, mine_ref, *(ref.at[0] for ref in whole_refs), kept_ref, sent_ref, kept_at, sent_at
    )


def second_kernel(kept_at, sent_at, x_ref, mine_ref, gate_ref, up_ref, down_ref, kept_ref, sent_ref):
    apply_rows(
        x_ref, mine_ref, gate_ref.at[0], up_ref.at[0], down_ref.at[0],
        kept_ref, sent_ref, kept_at, sent_at,
    )


def expert_rows(x_all, mine, weights, cap, first_block, blocks, kept_at, sent_at):
    members, _, extended = x_all.shape
    gathered = len(weights) == 1
    if gathered:
        tp_size, kinds, width, cols = weights[0].shape
        whole = (1, width, tp_size * cols)
    else:
        whole = weights[0].shape
        width = whole[1]

    def fixed(shape):
        return pl.BlockSpec(shape, lambda i: (0,) * len(shape))

    half = jax.ShapeDtypeStruct((members // 2, blocks * cap, width), jnp.bfloat16)
    half_spec = pl.BlockSpec((members // 2, cap, width), lambda i: (0, i, 0))
    extra = 3 if gathered else 0
    body = functools.partial(first_kernel if gathered else second_kernel, kept_at, sent_at)
    hidden = whole[2]
    return pl.pallas_call(
        body,
        grid=(blocks,),
        in_specs=[
            pl.BlockSpec((members, cap, extended), lambda i: (0, i + first_block, 0)),
            fixed(mine.shape),
        ]
        + [fixed(w.shape) for w in weights],
        out_specs=[half_spec] * 2 + [fixed(whole)] * extra,
        out_shape=[half] * 2 + [jax.ShapeDtypeStruct(whole, jnp.bfloat16)] * extra,
        compiler_params=pltpu.CompilerParams(vmem_limit_bytes=56 << 20),
        cost_estimate=pl.CostEstimate(
            flops=6 * members * blocks * cap * width * hidden,
            bytes_accessed=2 * (6 * width * hidden + 2 * members * blocks * cap * width),
            transcendentals=members * blocks * cap * hidden,
        ),
    )(x_all, mine, *weights)


def local(
    tokens, expert_group, expert_fine, route_weight, norm_gain, gate_master, up_master, down_master
):
    tok_rows, width = tokens.shape
    fs_size = lax.axis_size("fs")
    experts_all = gate_master.shape[0]
    groups = experts_all // FINE
    members = fs_size // groups
    cap = tok_rows // groups
    fs_me = lax.axis_index("fs")
    group_me, fine_me = fs_me // members, fs_me % members

    widened = tokens.astype(jnp.float32)
    normed = (
        widened * lax.rsqrt(jnp.mean(widened * widened, axis=-1, keepdims=True) + EPS)
    ).astype(jnp.bfloat16)
    away = (expert_group - group_me + groups) % groups
    index = jnp.arange(tok_rows, dtype=jnp.int32)
    same = (away[:, None] == away[None, :]) & (index[None, :] < index[:, None])
    slot = away * cap + jnp.sum(same.astype(jnp.int32), axis=1)
    placing = (index[:, None] == slot[None, :]).astype(jnp.bfloat16)
    fines = jnp.arange(FINE, dtype=jnp.int32)
    share = jnp.sum(
        jnp.where(expert_fine[:, None, :] == fines[None, :, None], route_weight[:, None, :], 0.0),
        axis=2,
    )
    high = lax.reduce_precision(share, 8, 7)
    middle = lax.reduce_precision(share - high, 8, 7)
    low = share - high - middle
    terms = jnp.concatenate([high, middle, low], axis=1).astype(jnp.bfloat16)
    terms = jnp.pad(terms, ((0, 0), (0, 128 - terms.shape[1])))
    extended = jnp.concatenate([normed, terms], axis=1)
    ordered = jnp.dot(placing, extended, preferred_element_type=jnp.float32).astype(jnp.bfloat16)

    pieces = jnp.stack(
        [norm_gain[None, :, None] * gate_master, norm_gain[None, :, None] * up_master, down_master],
        axis=1,
    ).astype(jnp.bfloat16)
    x_all, ready = gather(ordered, pieces, members, cap)
    lanes = jnp.arange(128, dtype=jnp.int32)
    mine = ((lanes % FINE == fine_me) & (lanes < 3 * FINE)).astype(jnp.float32)[None, :]

    def collect(kept, sent, first, second):
        far_part = flip(sent, "fs", second)
        pair = (kept.astype(jnp.float32) + far_part.astype(jnp.float32)).astype(jnp.bfloat16)
        back = flip(pair[1], "fs", first)
        return (pair[0].astype(jnp.float32) + back.astype(jnp.float32)).astype(jnp.bfloat16)

    kept, sent, gate_ready, up_ready, down_ready = expert_rows(
        x_all, mine, (ready,), cap, 1, groups - 1, (0, 2), (1, 3)
    )
    far_mixed = collect(kept, sent, 2, 1)
    kept, sent = expert_rows(
        x_all, mine, (gate_ready, up_ready, down_ready), cap, 0, 1, (0, 1), (2, 3)
    )
    near_mixed = collect(kept, sent, 1, 2)
    returned = [near_mixed] + [
        shift(far_mixed[(r - 1) * cap : r * cap], "fs", -r * members) for r in range(1, groups)
    ]
    mixed = lax.dot_general(
        placing,
        jnp.concatenate(returned),
        (((0,), (0,)), ((), ())),
        preferred_element_type=jnp.float32,
    ).astype(jnp.bfloat16)
    return (mixed, gate_ready, up_ready, down_ready)


def fused_kernel(
    groups, chips, cap, gain_ref, group_ref, fine_ref, weight_ref, tok_hbm, gate_hbm, up_hbm, down_hbm,
    place_out, ret_out, gate_out, up_out, down_out,
    master, tok, piece_gu, piece_dn, w_gu, w_dn, x_rows, far_rows, share, far_share, act,
    y_send, y_recv, part, z_send, ret, place,
    lsem, gsend, grecv, dsend, drecv, tsend, trecv, ysend, yrecv, zsend, zrecv,
):
    rows, cols = piece_gu.shape[4:]
    toks, width = tok.shape
    hidden = w_dn.shape[2]
    fs, tp = lax.axis_index("fs"), lax.axis_index("tp")
    group, bit, side = fs // FINE, (fs // 2) % 2, fs % 2
    chip, core = tp // 2, tp % 2
    bf16, f32 = jnp.bfloat16, jnp.float32

    def ahead(r):
        return (group + r) % groups

    def behind(r):
        return (group + groups - r) % groups

    def member(grp, bb, jj):
        return grp * FINE + (bit + bb - 2 * bit * bb) * 2 + (side + jj - 2 * side * jj)

    def flipped(a, b):
        return a + b - 2 * a * b

    def entry(grp):
        return 1 - grp % 2

    def source(r, bb, jj):
        grp = behind(r)
        if r == 0:
            return member(grp, bb, jj)
        return grp * FINE + flipped(entry(grp), bb) * 2 + flipped(side, jj)

    def chip_ahead(q):
        return (chip + q) % chips

    def chip_behind(q):
        return (chip + chips - q) % chips

    def block(f):
        return pl.ds(pl.multiple_of(f * rows, rows), rows)

    def lanes(t):
        return pl.ds(pl.multiple_of(t * cols, cols), cols)

    loads = []
    for k, (src, dst) in enumerate(
        ((gate_hbm, master.at[0]), (up_hbm, master.at[1]), (tok_hbm, tok), (down_hbm, master.at[2]))
    ):
        copy = pltpu.make_async_copy(src, dst, lsem.at[k])
        copy.start()
        loads.append(copy)

    links = [(member(group, 0, 1), tp), (member(group, 1, 0), tp)]
    links += [(ahead(r) * FINE + m, tp) for r in range(1, groups) for m in range(FINE)]
    links += [(fs, chip_ahead(q) * 2 + core) for q in range(1, chips)] + [(fs, chip * 2 + 1 - core)]
    barrier = pltpu.get_barrier_semaphore()
    for f, t in links:
        pl.semaphore_signal(
            barrier, inc=1, device_id={"fs": f, "tp": t}, device_id_type=pl.DeviceIdType.MESH
        )

    inner = bit == entry(group)
    outer = jnp.logical_not(inner)

    def remote(src, dst, send_sem, recv_sem, f, t):
        return pltpu.make_async_remote_copy(
            src_ref=src, dst_ref=dst, send_sem=send_sem, recv_sem=recv_sem,
            device_id={"fs": f, "tp": t}, device_id_type=pl.DeviceIdType.MESH,
        )

    gain = jnp.transpose(jnp.broadcast_to(gain_ref[...], (cols, rows)))
    loads[0].wait()
    loads[1].wait()
    experts_all = master.shape[1]
    for e in range(experts_all):
        for kind in (0, 1):
            piece_gu[e // FINE, e % 2, (e % FINE) // 2, kind] = (gain * master[kind, e]).astype(bf16)
    pl.semaphore_wait(barrier, len(links))

    count = 4 * groups
    keys = [(r, bb, jj) for r in range(groups) for bb in (0, 1) for jj in (0, 1)]

    class Route:
        def __init__(self, piece, whole, send_sem, recv_sem):
            self.piece, self.whole, self.lead = piece, whole, (slice(None),) * (len(whole.shape) - 2)
            self.send_sem, self.recv_sem = send_sem, recv_sem

        def region(self, f, t):
            return self.whole.at[self.lead + (block(f), lanes(t))]

        def move(self, src, dst, sent, received, f, t):
            return remote(src, dst, self.send_sem.at[sent], self.recv_sem.at[received], f, t)

        def src(self, key):
            return self.region(source(*key), tp) if any(key) else self.piece.at[group, side]

        def land(self, key):
            r, bb, jj = key
            k = keys.index(key)
            if key == (0, 0, 1):
                piece = self.piece.at[group, flipped(side, 1)]
                return self.move(piece, self.region(fs, tp), k, k, member(group, 0, 1), tp)
            first = key if r else (0, 0, jj)
            here = self.region(source(*first), tp)
            return self.move(self.src(first), here, k, k, member(group, 1, 0), tp)

        def direct(self, r, jj):
            j = flipped(side, jj)
            to = ahead(r) * FINE + entry(ahead(r)) * 2 + j
            slot = r * 4 + flipped(bit, entry(group)) * 2 + jj
            piece = self.piece.at[ahead(r), j]
            return self.move(piece, self.region(fs, tp), count + r * 2 + jj, slot, to, tp)

        def across(self, key, q):
            here = self.region(source(*key), tp)
            k = count + keys.index(key) * (chips - 1) + q - 1
            return self.move(self.src(key), here, k + 2 * groups, k, fs, chip_ahead(q) * 2 + core)

        def beside(self, key, q):
            here = self.region(source(*key), chip_behind(q) * 2 + core)
            src = self.src(key) if q == 0 else here
            k = count * chips + keys.index(key) * chips + q
            return self.move(src, here, k + 2 * groups, k, fs, chip * 2 + 1 - core)

        def hand(self, key):
            for q in range(1, chips):
                self.across(key, q).start()
            self.beside(key, 0).start()

        def arrived(self, key, forward=False):
            self.land(key).wait_recv()
            if forward:
                self.land(key).start()
            if key == (0, 0, 1):
                self.land((0, 1, 1)).start()
            self.hand(key)

        def crossed(self, key):
            for q in range(1, chips):
                self.across(key, q).wait_recv()
                self.beside(key, q).start()

        def directs(self):
            for r in range(1, groups):
                for jj in (0, 1):
                    self.direct(r, jj).start()

        def drain(self):
            for key in keys:
                if any(key) and not key[0]:
                    self.land(key).wait_send()
                for q in range(chips):
                    if q:
                        self.across(key, q).wait_send()
                    self.beside(key, q).wait_send()
            for r in range(1, groups):
                for jj in (0, 1):
                    self.direct(r, jj).wait_send()

            @pl.when(inner)
            def _():
                for key in keys[4:]:
                    self.land(key).wait_send()

    gu = Route(piece_gu, w_gu, gsend, grecv)
    dn = Route(piece_dn, w_dn, dsend, drecv)

    gu.land((0, 0, 1)).start()
    gu.land((0, 1, 0)).start()
    gu.hand((0, 0, 0))
    pl.when(inner)(gu.directs)
    keep_gu = pltpu.make_async_copy(piece_gu.at[group, side], gu.region(fs, tp), lsem.at[4])
    keep_gu.start()

    loads[2].wait()
    pad = max(8, groups)
    away = group_ref[...] - group
    away = jnp.where(away < 0, away + groups, away)
    which = lax.broadcasted_iota(jnp.int32, (pad, toks), 0)
    mine = (which == away).astype(f32)
    first = lax.broadcasted_iota(jnp.int32, (toks, toks), 0)
    second = lax.broadcasted_iota(jnp.int32, (toks, toks), 1)
    before = jnp.dot(
        mine.astype(bf16), (first < second).astype(f32).astype(bf16), preferred_element_type=f32
    )
    slot = jnp.sum(mine * (before + (which * cap).astype(f32)), axis=0, keepdims=True)
    placing = (first.astype(f32) == slot).astype(f32)
    place[...] = placing.astype(bf16)
    finer = lax.broadcasted_iota(jnp.int32, (8, toks), 0)
    shares = jnp.zeros((8, toks), f32)
    for k in range(fine_ref.shape[0]):
        shares += jnp.where(finer == fine_ref[k : k + 1, :], weight_ref[k : k + 1, :], 0.0)
    shares = lax.dot_general(
        shares, placing, (((1,), (1,)), ((), ())),
        preferred_element_type=f32, precision=lax.Precision.HIGHEST,
    )

    def normed(r):
        raw = jnp.dot(place[r * cap : (r + 1) * cap, :], tok[...], preferred_element_type=f32)
        scale = lax.rsqrt(jnp.mean(raw * raw, axis=1, keepdims=True) + EPS)
        return (raw * scale).astype(bf16)

    def at(r, jj):
        return pl.ds((r * 2 + jj) * cap, cap)

    share[0, 0] = shares[:, :cap]
    for r in range(1, groups):
        far_share[r - 1] = shares[:, r * cap : (r + 1) * cap]
    x_rows[at(0, 0), :] = normed(0)
    mate = member(group, 0, 1)
    parts = 2
    step = cap // parts

    def rows_move(k, src, dst, f):
        return remote(src, dst, tsend.at[k], trecv.at[k], f, tp)

    def near():
        return [
            rows_move(0, share.at[0, 0], share.at[0, 1], mate),
            rows_move(1, x_rows.at[at(0, 0)], x_rows.at[at(0, 1)], mate),
        ]

    def far(r):
        to, base = member(ahead(r), 0, 0), 2 + (r - 1) * 2 * (parts + 1)
        moves = [rows_move(base, far_share.at[r - 1], share.at[r, 0], to)]
        for p in range(parts):
            here = pl.ds(r * 2 * cap + p * step, step)
            src = far_rows.at[r - 1, pl.ds(p * step, step)]
            moves.append(rows_move(base + 1 + p, src, x_rows.at[here], to))
        return moves

    def passed(r):
        base = 2 + (r - 1) * 2 * (parts + 1) + parts + 1
        moves = [rows_move(base, share.at[r, 0], share.at[r, 1], mate)]
        for p in range(parts):
            here = pl.ds(r * 2 * cap + p * step, step)
            there = pl.ds((r * 2 + 1) * cap + p * step, step)
            moves.append(rows_move(base + 1 + p, x_rows.at[here], x_rows.at[there], mate))
        return moves

    def start_far():
        for r in range(1, groups):
            for move in far(r):
                move.start()

    def pass_far():
        for r in range(1, groups):
            for landed, move in zip(far(r), passed(r)):
                landed.wait_recv()
                move.start()

    for move in near():
        move.start()
    for r in range(1, groups):
        far_rows[r - 1] = normed(r)

    loads[3].wait()
    for e in range(experts_all):
        piece_dn[e // FINE, e % 2, (e % FINE) // 2] = master[2, e].astype(bf16)
    keep_dn = pltpu.make_async_copy(piece_dn.at[group, side], dn.region(fs, tp), lsem.at[5])
    keep_dn.start()
    others = range(1, groups)
    inner_order = [(0, 0, 0), (0, 1, 0), (0, 0, 1)]
    inner_order += [(r, 0, jj) for r in others for jj in (0, 1)] + [(0, 1, 1)]
    inner_order += [(r, 1, jj) for r in others for jj in (0, 1)]
    outer_order = [(0, 0, 0), (0, 0, 1), (0, 1, 0), (0, 1, 1)]
    outer_order += [(r, bb, jj) for r in others for bb in (0, 1) for jj in (0, 1)]
    ahead_of = 3

    def route_gates(order, forward):
        done = 0
        for k, key in enumerate(order[1:]):
            gu.arrived(key, forward and key[0] > 0)
            if key == (0, 0, 1):
                dn.land((0, 0, 1)).start()
                dn.beside((0, 0, 0), 0).start()
                if not forward:
                    gu.directs()
                    start_far()
            if k >= ahead_of:
                gu.crossed(order[done])
                done += 1
        if forward:
            start_far()
        for q in range(1, chips):
            dn.across((0, 0, 0), q).start()

    pl.when(inner)(lambda: route_gates(inner_order, True))
    pl.when(outer)(lambda: route_gates(outer_order, False))

    def apply_rows(start, count, s, lane0, lane_count):
        here = pl.ds(start * cap, count * cap)
        x = x_rows[here, :]
        at_lanes = pl.ds(pl.multiple_of(lane0, cols), lane_count)
        gate_value = jnp.dot(x, w_gu[s, 0, :, at_lanes], preferred_element_type=f32)
        upward = jnp.dot(x, w_gu[s, 1, :, at_lanes], preferred_element_type=f32)
        fine = s * 2 + side
        chosen = []
        for i in range(start, start + count):
            flat = jnp.transpose(share[i // 2, i % 2])
            lane = lax.broadcasted_iota(jnp.int32, flat.shape, 1)
            chosen.append(jnp.sum(jnp.where(lane == fine, flat, 0.0), axis=1, keepdims=True))
        weight = jnp.concatenate(chosen, axis=0)
        value = gate_value / (1.0 + jnp.exp(-gate_value)) * upward * weight
        act[here, pl.ds(pl.multiple_of(s * hidden + lane0, cols), lane_count)] = value.astype(bf16)

    keep_gu.wait()
    for key in keys:
        if any(key):
            gu.beside(key, 0).wait_recv()
    gu.beside((0, 0, 0), 0).wait_recv()
    for move in near():
        move.wait_recv()
    pair = 2 * cols
    for s in (0, 1):
        apply_rows(0, 2, s, chip * pair, pair)

    def finish_gates(order, forward):
        rest = order[len(order) - 1 - ahead_of :]
        dn.land((0, 0, 1)).wait_recv()
        dn.hand((0, 0, 1))
        if not forward:
            dn.land((0, 1, 0)).start()
            dn.land((0, 1, 1)).start()
        for k, key in enumerate(rest):
            if k == len(rest) - (2 if forward else 2):
                pass_far()
            if k == len(rest) - (0 if forward else 1):
                if forward:
                    dn.land((0, 1, 0)).start()
                    dn.land((0, 1, 1)).start()
                dn.directs()
            gu.crossed(key)
        if forward:
            dn.land((0, 1, 0)).start()
            dn.land((0, 1, 1)).start()
            dn.directs()

    pl.when(inner)(lambda: finish_gates(inner_order, True))
    pl.when(outer)(lambda: finish_gates(outer_order, False))
    for key in keys:
        for q in range(1, chips):
            gu.beside(key, q).wait_recv()
    for q in range(1, chips):
        for s in (0, 1):
            apply_rows(0, 2, s, chip_behind(q) * pair, pair)
    outs = [
        pltpu.make_async_copy(w_gu.at[bit, 0], gate_out.at[0], lsem.at[6]),
        pltpu.make_async_copy(w_gu.at[bit, 1], up_out.at[0], lsem.at[7]),
    ]
    for copy in outs:
        copy.start()

    keep_dn.wait()
    span = 2 * rows
    steps = [(0, 0), (0, 1)] + [(r, bb) for r in range(1, groups) for bb in (1, 0)]

    def columns(n, cut, cuts, base=group):
        r, bb = steps[n]
        wide = span // cuts
        grp = (base + groups - r) % groups
        pick = flipped(entry(grp) if r else bit, bb)
        start = (grp * FINE + pick * 2) * rows + cut * wide
        return pl.ds(pl.multiple_of(start, wide), wide)

    crossing, home = {}, {}

    def ready(n):
        r, bb = steps[n]
        for jj in (0, 1):
            for q in range(chips):
                dn.beside((r, bb, jj), q).wait_recv()

    def produce(n, r, cut, cuts):
        here = columns(n, cut, cuts)
        mine = pl.ds(r * 2 * cap, 2 * cap)
        out = jnp.zeros((2 * cap, span // cuts), f32)
        for s in (0, 1):
            out += lax.dot_general(
                act[mine, s * hidden : (s + 1) * hidden], w_dn[s, here, :],
                (((1,), (1,)), ((), ())), preferred_element_type=f32,
            )
        y_send[r, :, here] = out[cap:].astype(bf16)
        part[r, :, here] = out[:cap]
        k = len(crossing)
        crossing[n, r, cut, cuts] = remote(
            y_send.at[r, :, here], y_recv.at[r, :, here], ysend.at[k], yrecv.at[k], mate, tp
        )
        crossing[n, r, cut, cuts].start()
        waiting.append((n, r, cut, cuts))

    def combine(n, r, cut, cuts):
        here = columns(n, cut, cuts)
        crossing[n, r, cut, cuts].wait_recv()
        total = (part[r, :, here] + y_recv[r, :, here].astype(f32)).astype(bf16)
        if r == 0:
            ret[0, :, here] = total
        else:
            z_send[r - 1, :, here] = total
            k = len(home)
            home[n, r, cut] = remote(
                z_send.at[r - 1, :, here], ret.at[r, :, here], zsend.at[k], zrecv.at[k],
                member(behind(r), 0, 0), tp,
            )
            home[n, r, cut].start()

    waiting = []
    last = len(steps) - 1

    def cuts_of(n):
        return 2 if n in (last,) else 1


    def far_down(bb):
        for r in others:
            for jj in (0, 1):
                dn.arrived((r, bb, jj), True)

    def far_down_outer(bb):
        for r in others:
            for jj in (0, 1):
                dn.arrived((r, bb, jj))

    def near_down():
        dn.arrived((0, 1, 0))
        dn.arrived((0, 1, 1))

    pl.when(outer)(near_down)
    for r in others:
        for move in passed(r):
            move.wait_recv()
        for s in (0, 1):
            for half in range(chips):
                apply_rows(2 * r, 2, s, half * pair, pair)
    pl.when(inner)(near_down)
    for jj in (0, 1):
        dn.crossed((0, 0, jj))
    pl.when(inner)(lambda: far_down(1))
    ready(0)
    for r in reversed(range(groups)):
        for cut in range(cuts_of(0)):
            produce(0, r, cut, cuts_of(0))
    pl.when(outer)(lambda: far_down_outer(1))
    pl.when(inner)(lambda: far_down(0))
    def settle(far_only):
        for item in [w for w in waiting if w[1] or not far_only]:
            waiting.remove(item)
            combine(*item)

    for n in range(1, len(steps)):
        for jj in (0, 1):
            dn.crossed((*steps[n], jj))
        settle(True)
        if n == 2:
            pl.when(outer)(lambda: far_down_outer(0))
        ready(n)
        for r in reversed(range(groups)):
            for cut in range(cuts_of(n)):
                produce(n, r, cut, cuts_of(n))
            if r == 1:
                for item in [w for w in waiting if w[0] < n]:
                    waiting.remove(item)
                    combine(*item)
    outs.append(pltpu.make_async_copy(w_dn.at[bit], down_out.at[0], lsem.at[8]))
    outs[-1].start()
    outs.append(pltpu.make_async_copy(place, place_out, lsem.at[10]))
    outs[-1].start()
    settle(True)
    settle(False)
    outs.append(pltpu.make_async_copy(ret.at[0], ret_out.at[0], lsem.at[9]))
    outs[-1].start()
    gu.drain()
    dn.drain()
    for move in near():
        move.wait_send()
    for r in others:
        for move in far(r) + passed(r):
            move.wait_send()
    for k, ((n, r, cut), copy) in enumerate(home.items()):
        copy.wait_recv()
        here = columns(n, cut, cuts_of(n), ahead(r))
        outs.append(
            pltpu.make_async_copy(ret.at[r, :, here], ret_out.at[r, :, here], lsem.at[11 + k])
        )
        outs[-1].start()
    for copy in list(crossing.values()) + list(home.values()):
        copy.wait_send()
    for copy in outs:
        copy.wait()


def publish_kernel(
    place_ref, ret_ref, gate_ref, up_ref, down_ref, mixed_out, gate_out, up_out, down_out,
    mixed, out_sem, row_sem,
):
    writes = [
        pltpu.make_async_copy(src, dst, out_sem.at[k])
        for k, (src, dst) in enumerate(
            ((gate_ref, gate_out), (up_ref, up_out), (down_ref, down_out))
        )
    ]
    for write in writes:
        write.start()
    width = ret_ref.shape[1]
    chunk = min(width, 512)
    for c in range(0, width, chunk):
        here = pl.ds(c, chunk)
        mixed[:, here] = lax.dot_general(
            place_ref[...], ret_ref[:, here], (((0,), (0,)), ((), ())),
            preferred_element_type=jnp.float32,
        ).astype(jnp.bfloat16)
    last = pltpu.make_async_copy(mixed, mixed_out, row_sem)
    last.start()
    last.wait()
    for write in writes:
        write.wait()


def publish(placed, returned, gate, up, down):
    toks, width = returned.shape
    anywhere = pl.BlockSpec(memory_space=pl.ANY)
    local_spec = pl.BlockSpec(memory_space=pltpu.VMEM)
    whole = jax.ShapeDtypeStruct(gate.shape, gate.dtype)
    return pl.pallas_call(
        publish_kernel,
        out_shape=(jax.ShapeDtypeStruct((toks, width), returned.dtype), whole, whole, whole),
        in_specs=[local_spec] * 2 + [anywhere] * 3,
        out_specs=(anywhere,) * 4,
        scratch_shapes=[
            pltpu.VMEM((toks, width), returned.dtype),
            pltpu.SemaphoreType.DMA((3,)),
            pltpu.SemaphoreType.DMA,
        ],
        compiler_params=pltpu.CompilerParams(vmem_limit_bytes=12 << 20),
        cost_estimate=pl.CostEstimate(
            flops=2 * toks * toks * width, bytes_accessed=6 * gate.size * 2, transcendentals=0
        ),
    )(placed, returned, gate, up, down)


def fused(
    tokens, expert_group, expert_fine, route_weight, norm_gain, gate_master, up_master, down_master
):
    toks, width = tokens.shape
    fs_size, tp_size = lax.axis_size("fs"), lax.axis_size("tp")
    experts_all, rows, cols = gate_master.shape
    groups, chips, hidden = experts_all // FINE, tp_size // 2, cols * tp_size
    cap = toks // groups
    bf16, f32 = jnp.bfloat16, jnp.float32
    sources = groups * 4
    sends = sources * 2 * chips + 2 * groups
    moves = 2 + (groups - 1) * 6
    steps = 2 * groups
    vmem, dma = pltpu.VMEM, pltpu.SemaphoreType.DMA
    anywhere = pl.BlockSpec(memory_space=pl.ANY)
    local_spec = pl.BlockSpec(memory_space=pltpu.VMEM)
    sent = 2 * (3 * width * hidden * 2 + 6 * toks * width)
    placed, returned, *ready = pl.pallas_call(
        functools.partial(fused_kernel, groups, chips, cap),
        out_shape=(
            vmem((toks, toks), bf16),
            vmem((groups, cap, width), bf16),
            vmem((1, width, hidden), bf16),
            vmem((1, width, hidden), bf16),
            vmem((1, width, hidden), bf16),
        ),
        in_specs=[local_spec] * 4 + [pl.BlockSpec(memory_space=pltpu.HBM)] * 4,
        out_specs=(anywhere,) * 5,
        scratch_shapes=[
            vmem((3, experts_all, rows, cols), f32),
            vmem((toks, width), bf16),
            vmem((groups, 2, 2, 2, rows, cols), bf16),
            vmem((groups, 2, 2, rows, cols), bf16),
            vmem((2, 2, width, hidden), bf16),
            vmem((2, width, hidden), bf16),
            vmem((2 * groups * cap, width), bf16),
            vmem((groups - 1, cap, width), bf16),
            vmem((groups, 2, 8, cap), f32),
            vmem((groups - 1, 8, cap), f32),
            vmem((2 * groups * cap, 2 * hidden), bf16),
            vmem((groups, cap, width), bf16),
            vmem((groups, cap, width), bf16),
            vmem((groups, cap, width), f32),
            vmem((groups - 1, cap, width), bf16),
            vmem((groups, cap, width), bf16),
            vmem((toks, toks), bf16),
            dma((11 + (steps + 2) * (groups - 1),)),
            dma((sends,)), dma((sends,)), dma((sends,)), dma((sends,)),
            dma((moves,)), dma((moves,)),
            dma(((steps + 2) * groups,)), dma(((steps + 2) * groups,)),
            dma(((steps + 2) * (groups - 1),)), dma(((steps + 2) * (groups - 1),)),
        ],
        compiler_params=pltpu.CompilerParams(
            collective_id=1, has_side_effects=True, vmem_limit_bytes=56 << 20
        ),
        cost_estimate=pl.CostEstimate(
            flops=12 * groups * cap * 2 * width * hidden, bytes_accessed=sent, transcendentals=0
        ),
    )(
        norm_gain[None, :], expert_group[None, :], expert_fine.T, route_weight.T,
        tokens, gate_master, up_master, down_master,
    )
    return publish(placed, returned.reshape(toks, width), *ready)


def step(*args):
    tp_size = lax.axis_size("tp")
    gate_master = args[5]
    groups = gate_master.shape[0] // FINE
    if lax.axis_size("fs") == gate_master.shape[0] and tp_size > 2 and groups > 1 and gate_master.shape[2] % 128 == 0:
        return fused(*args)
    return local(*args)


def solution(mesh):
    in_specs = (
        P(("fs", "tp"), None),
        P(("fs", "tp")),
        P(("fs", "tp"), None),
        P(("fs", "tp"), None),
        P("fs"),
        P(None, "fs", "tp"),
        P(None, "fs", "tp"),
        P(None, "fs", "tp"),
    )
    out_specs = (
        P(("fs", "tp"), None),
        P("fs", None, None),
        P("fs", None, None),
        P("fs", None, None),
    )
    return jax.shard_map(step, mesh=mesh, in_specs=in_specs, out_specs=out_specs, check_vma=False)
```

```python
import functools

import jax
import jax.numpy as jnp
from jax import lax
from jax.experimental import pallas as pl
from jax.experimental.pallas import tpu as pltpu
from jax.sharding import PartitionSpec as P

FINE = 4


EPS = 1e-06


def flip(value, axis, bit):
    size = lax.axis_size(axis)
    return lax.ppermute(value, axis, [(i, i ^ bit) for i in range(size)])


def shift(value, axis, step):
    size = lax.axis_size(axis)
    return lax.ppermute(value, axis, [(i, (i + step) % size) for i in range(size)])


def gather_kernel(
    fs_size, tp_size, members, cap, tok_ref, piece_ref, x_ref, ready_ref,
    local_sem, tsend, trecv, psend, precv, xsend, xrecv, csend, crecv,
):
    groups, chips = fs_size // members, tp_size // 2
    tok_rows = tok_ref.shape[0]
    rows = piece_ref.shape[2]
    fs, tp = lax.axis_index("fs"), lax.axis_index("tp")
    group, member = fs // members, fs % members
    chip, core = tp // 2, tp % 2

    def away(r, i):
        base = member + i - 2 * (member & i)
        ahead = ((group + r) % groups) * members + base
        behind = ((group + groups - r) % groups) * members + base
        return ahead, behind

    def chip_tp(q, c):
        return ((chip + q) % chips) * 2 + c

    peers = [
        (away(r, i)[0], tp) for r in range(groups) for i in range(members) if r or i
    ]
    peers += [(fs, chip_tp(q, core)) for q in range(1, chips)] + [(fs, chip_tp(0, 1 - core))]
    barrier = pltpu.get_barrier_semaphore()
    for f, t in peers:
        pl.semaphore_signal(
            barrier, inc=1, device_id={"fs": f, "tp": t}, device_id_type=pl.DeviceIdType.MESH
        )
    pl.semaphore_wait(barrier, len(peers))

    started = []

    def send(src, dst, send_sem, recv_sem, f, t):
        copy = pltpu.make_async_remote_copy(
            src_ref=src, dst_ref=dst, send_sem=send_sem, recv_sem=recv_sem,
            device_id={"fs": f, "tp": t}, device_id_type=pl.DeviceIdType.MESH,
        )
        copy.start()
        started.append(copy)
        return copy

    near, far = pl.ds(0, cap), pl.ds(cap, tok_rows - cap)

    def pass_on(src, part, j, bit, k):
        return send(
            src, x_ref.at[j, part], tsend.at[k], trecv.at[k], away(0, bit)[0], tp
        )

    def block(f):
        return pl.ds(pl.multiple_of(f * rows, rows), rows)

    near_2 = pass_on(tok_ref.at[near], near, 2, 2, 0)
    near_1 = pass_on(tok_ref.at[near], near, 1, 1, 1)
    crossing = []
    for r in range(1, groups):
        part = pl.ds(r * cap, cap)
        crossing.append(
            send(tok_ref.at[part], x_ref.at[0, part], tsend.at[5 + r], trecv.at[5 + r], away(r, 0)[0], tp)
        )
    kept = pltpu.make_async_copy(tok_ref.at[near], x_ref.at[0, near], local_sem.at[0])
    kept.start()
    own = pltpu.make_async_copy(piece_ref.at[fs], ready_ref.at[tp, :, block(fs)], local_sem.at[1])
    own.start()

    pieces = {}
    for r in range(groups):
        for i in range(members):
            if r or i:
                k = r * members + i
                to = away(r, i)[0]
                pieces[r, i] = send(
                    piece_ref.at[to], ready_ref.at[tp, :, block(fs)], psend.at[k], precv.at[k], to, tp
                )
    own.wait()
    across = {}

    def cross_chips(r, i):
        here = ready_ref.at[tp, :, block(away(r, i)[1])]
        for q in range(1, chips):
            k = r * members + i
            across[q, r, i] = send(
                here, here, xsend.at[q - 1, k], xrecv.at[q - 1, k], fs, chip_tp(q, core)
            )

    beside = []

    def cross_cores(q, r):
        size = members * rows
        start = ((group + groups - r) % groups) * size
        here = ready_ref.at[chip_tp(chips - q, core), :, pl.ds(pl.multiple_of(start, size), size)]
        beside.append(
            send(here, here, csend.at[q, r], crecv.at[q, r], fs, chip_tp(0, 1 - core))
        )

    cross_chips(0, 0)
    for i in range(1, members):
        pieces[0, i].wait_recv()
        cross_chips(0, i)
    cross_cores(0, 0)
    near_2.wait_recv()
    near_3 = pass_on(x_ref.at[2, near], near, 3, 1, 2)
    for copy in crossing:
        copy.wait_recv()
    far_2 = pass_on(x_ref.at[0, far], far, 2, 2, 3)
    far_1 = pass_on(x_ref.at[0, far], far, 1, 1, 4)
    passed = False
    for r in range(1, groups):
        for i in range(members):
            pieces[r, i].wait_recv()
            cross_chips(r, i)
            if not passed and i == members // 2 - 1:
                passed = True
                far_2.wait_recv()
                far_3 = pass_on(x_ref.at[2, far], far, 3, 1, 5)
        cross_cores(0, r)
    for r in range(groups):
        for q in range(1, chips):
            for i in range(members):
                across[q, r, i].wait_recv()
            cross_cores(q, r)
    near_1.wait_recv()
    near_3.wait_recv()
    far_1.wait_recv()
    far_3.wait_recv()
    for copy in beside:
        copy.wait_recv()
    kept.wait()
    for copy in started:
        copy.wait_send()


def gather(ordered, pieces, members, cap):
    fs_size, tp_size = lax.axis_size("fs"), lax.axis_size("tp")
    experts_all, kinds, rows, cols = pieces.shape
    chips = tp_size // 2
    moves, crossings = 6, fs_size // members - 1
    dma = pltpu.SemaphoreType.DMA
    sent = 5 * ordered.size + 3 * pieces.size
    return pl.pallas_call(
        functools.partial(gather_kernel, fs_size, tp_size, members, cap),
        out_shape=(
            jax.ShapeDtypeStruct((members,) + ordered.shape, ordered.dtype),
            jax.ShapeDtypeStruct((tp_size, kinds, fs_size * rows, cols), pieces.dtype),
        ),
        in_specs=[pl.BlockSpec(memory_space=pltpu.VMEM)] * 2,
        out_specs=(pl.BlockSpec(memory_space=pl.ANY),) * 2,
        scratch_shapes=[
            dma((2,)),
            dma((moves + crossings,)),
            dma((moves + crossings,)),
            dma((fs_size,)),
            dma((fs_size,)),
            dma((max(chips - 1, 1), fs_size)),
            dma((max(chips - 1, 1), fs_size)),
            dma((chips, fs_size // members)),
            dma((chips, fs_size // members)),
        ],
        compiler_params=pltpu.CompilerParams(collective_id=0, has_side_effects=True),
        cost_estimate=pl.CostEstimate(flops=0, bytes_accessed=4 * sent, transcendentals=0),
    )(ordered, pieces)


def apply_rows(x_ref, mine_ref, gate_ref, up_ref, down_ref, kept_ref, sent_ref, kept_at, sent_at):
    members, cap, _ = x_ref.shape
    width, _ = gate_ref.shape
    x = x_ref[:, :, :width].reshape(members * cap, width)
    parts = x_ref[:, :, width:].reshape(members * cap, -1).astype(jnp.float32)
    weight = jnp.sum(parts * mine_ref[...], axis=1, keepdims=True)
    gate_value = jnp.dot(x, gate_ref[...], preferred_element_type=jnp.float32)
    upward = jnp.dot(x, up_ref[...], preferred_element_type=jnp.float32)
    activation = (gate_value / (1.0 + jnp.exp(-gate_value)) * upward).astype(jnp.bfloat16)
    step = min(width, 512)
    for at in range(0, width, step):
        out = lax.dot_general(
            activation,
            down_ref[at : at + step, :],
            (((1,), (1,)), ((), ())),
            preferred_element_type=jnp.float32,
        )
        out = (weight * out).astype(jnp.bfloat16)
        for ref, places in ((kept_ref, kept_at), (sent_ref, sent_at)):
            for i, j in enumerate(places):
                ref[i, :, at : at + step] = out[j * cap : (j + 1) * cap]


def first_kernel(kept_at, sent_at, x_ref, mine_ref, ready_ref, kept_ref, sent_ref, *whole_refs):
    @pl.when(pl.program_id(0) == 0)
    def _():
        cols = ready_ref.shape[3]
        for kind, ref in enumerate(whole_refs):
            for t in range(ready_ref.shape[0]):
                ref[0, :, t * cols : (t + 1) * cols] = ready_ref[t, kind]

    apply_rows(
        x_ref, mine_ref, *(ref.at[0] for ref in whole_refs), kept_ref, sent_ref, kept_at, sent_at
    )


def second_kernel(kept_at, sent_at, x_ref, mine_ref, gate_ref, up_ref, down_ref, kept_ref, sent_ref):
    apply_rows(
        x_ref, mine_ref, gate_ref.at[0], up_ref.at[0], down_ref.at[0],
        kept_ref, sent_ref, kept_at, sent_at,
    )


def expert_rows(x_all, mine, weights, cap, first_block, blocks, kept_at, sent_at):
    members, _, extended = x_all.shape
    gathered = len(weights) == 1
    if gathered:
        tp_size, kinds, width, cols = weights[0].shape
        whole = (1, width, tp_size * cols)
    else:
        whole = weights[0].shape
        width = whole[1]

    def fixed(shape):
        return pl.BlockSpec(shape, lambda i: (0,) * len(shape))

    half = jax.ShapeDtypeStruct((members // 2, blocks * cap, width), jnp.bfloat16)
    half_spec = pl.BlockSpec((members // 2, cap, width), lambda i: (0, i, 0))
    extra = 3 if gathered else 0
    body = functools.partial(first_kernel if gathered else second_kernel, kept_at, sent_at)
    hidden = whole[2]
    return pl.pallas_call(
        body,
        grid=(blocks,),
        in_specs=[
            pl.BlockSpec((members, cap, extended), lambda i: (0, i + first_block, 0)),
            fixed(mine.shape),
        ]
        + [fixed(w.shape) for w in weights],
        out_specs=[half_spec] * 2 + [fixed(whole)] * extra,
        out_shape=[half] * 2 + [jax.ShapeDtypeStruct(whole, jnp.bfloat16)] * extra,
        compiler_params=pltpu.CompilerParams(vmem_limit_bytes=56 << 20),
        cost_estimate=pl.CostEstimate(
            flops=6 * members * blocks * cap * width * hidden,
            bytes_accessed=2 * (6 * width * hidden + 2 * members * blocks * cap * width),
            transcendentals=members * blocks * cap * hidden,
        ),
    )(x_all, mine, *weights)


def local(
    tokens, expert_group, expert_fine, route_weight, norm_gain, gate_master, up_master, down_master
):
    tok_rows, width = tokens.shape
    fs_size = lax.axis_size("fs")
    experts_all = gate_master.shape[0]
    groups = experts_all // FINE
    members = fs_size // groups
    cap = tok_rows // groups
    fs_me = lax.axis_index("fs")
    group_me, fine_me = fs_me // members, fs_me % members

    widened = tokens.astype(jnp.float32)
    normed = (
        widened * lax.rsqrt(jnp.mean(widened * widened, axis=-1, keepdims=True) + EPS)
    ).astype(jnp.bfloat16)
    away = (expert_group - group_me + groups) % groups
    index = jnp.arange(tok_rows, dtype=jnp.int32)
    same = (away[:, None] == away[None, :]) & (index[None, :] < index[:, None])
    slot = away * cap + jnp.sum(same.astype(jnp.int32), axis=1)
    placing = (index[:, None] == slot[None, :]).astype(jnp.bfloat16)
    fines = jnp.arange(FINE, dtype=jnp.int32)
    share = jnp.sum(
        jnp.where(expert_fine[:, None, :] == fines[None, :, None], route_weight[:, None, :], 0.0),
        axis=2,
    )
    high = lax.reduce_precision(share, 8, 7)
    middle = lax.reduce_precision(share - high, 8, 7)
    low = share - high - middle
    terms = jnp.concatenate([high, middle, low], axis=1).astype(jnp.bfloat16)
    terms = jnp.pad(terms, ((0, 0), (0, 128 - terms.shape[1])))
    extended = jnp.concatenate([normed, terms], axis=1)
    ordered = jnp.dot(placing, extended, preferred_element_type=jnp.float32).astype(jnp.bfloat16)

    pieces = jnp.stack(
        [norm_gain[None, :, None] * gate_master, norm_gain[None, :, None] * up_master, down_master],
        axis=1,
    ).astype(jnp.bfloat16)
    x_all, ready = gather(ordered, pieces, members, cap)
    lanes = jnp.arange(128, dtype=jnp.int32)
    mine = ((lanes % FINE == fine_me) & (lanes < 3 * FINE)).astype(jnp.float32)[None, :]

    def collect(kept, sent, first, second):
        far_part = flip(sent, "fs", second)
        pair = (kept.astype(jnp.float32) + far_part.astype(jnp.float32)).astype(jnp.bfloat16)
        back = flip(pair[1], "fs", first)
        return (pair[0].astype(jnp.float32) + back.astype(jnp.float32)).astype(jnp.bfloat16)

    kept, sent, gate_ready, up_ready, down_ready = expert_rows(
        x_all, mine, (ready,), cap, 1, groups - 1, (0, 2), (1, 3)
    )
    far_mixed = collect(kept, sent, 2, 1)
    kept, sent = expert_rows(
        x_all, mine, (gate_ready, up_ready, down_ready), cap, 0, 1, (0, 1), (2, 3)
    )
    near_mixed = collect(kept, sent, 1, 2)
    returned = [near_mixed] + [
        shift(far_mixed[(r - 1) * cap : r * cap], "fs", -r * members) for r in range(1, groups)
    ]
    mixed = lax.dot_general(
        placing,
        jnp.concatenate(returned),
        (((0,), (0,)), ((), ())),
        preferred_element_type=jnp.float32,
    ).astype(jnp.bfloat16)
    return (mixed, gate_ready, up_ready, down_ready)


def fused_kernel(
    groups, chips, cap, gain_hbm, group_hbm, fine_hbm, weight_hbm, tok_hbm, gate_hbm, up_hbm, down_hbm,
    place_out, ret_out, gate_out, up_out, down_out,
    master, tok, piece_gu, piece_dn, w_gu, w_dn, x_rows, far_rows, share, far_share, act,
    y_send, y_recv, part, z_send, ret, place, gain_ref, group_ref, fine_ref, weight_ref,
    ssem, lsem, gsend, grecv, dsend, drecv, tsend, trecv, ysend, yrecv, zsend, zrecv,
):
    rows, cols = piece_gu.shape[4:]
    toks, width = tok.shape
    hidden = w_dn.shape[2]
    fs, tp = lax.axis_index("fs"), lax.axis_index("tp")
    group, bit, side = fs // FINE, (fs // 2) % 2, fs % 2
    chip, core = tp // 2, tp % 2
    bf16, f32 = jnp.bfloat16, jnp.float32

    def ahead(r):
        return (group + r) % groups

    def behind(r):
        return (group + groups - r) % groups

    def member(grp, bb, jj):
        return grp * FINE + (bit + bb - 2 * bit * bb) * 2 + (side + jj - 2 * side * jj)

    def flipped(a, b):
        return a + b - 2 * a * b

    def entry(grp):
        return 1 - grp % 2

    def source(r, bb, jj):
        grp = behind(r)
        if r == 0:
            return member(grp, bb, jj)
        return grp * FINE + flipped(entry(grp), bb) * 2 + flipped(side, jj)

    def chip_ahead(q):
        return (chip + q) % chips

    def chip_behind(q):
        return (chip + chips - q) % chips

    def block(f):
        return pl.ds(pl.multiple_of(f * rows, rows), rows)

    def lanes(t):
        return pl.ds(pl.multiple_of(t * cols, cols), cols)

    small = []
    for k, (src, dst) in enumerate(
        (
            (gain_hbm, gain_ref), (group_hbm, group_ref),
            (fine_hbm, fine_ref), (weight_hbm, weight_ref),
        )
    ):
        copy = pltpu.make_async_copy(src, dst, ssem.at[k])
        copy.start()
        small.append(copy)
    loads = []
    for k, (src, dst) in enumerate(
        ((gate_hbm, master.at[0]), (up_hbm, master.at[1]), (tok_hbm, tok), (down_hbm, master.at[2]))
    ):
        loads.append(pltpu.make_async_copy(src, dst, lsem.at[k]))
    loads[0].start()
    loads[1].start()

    links = [(member(group, 0, 1), tp), (member(group, 1, 0), tp)]
    links += [(ahead(r) * FINE + m, tp) for r in range(1, groups) for m in range(FINE)]
    links += [(fs, chip_ahead(q) * 2 + core) for q in range(1, chips)] + [(fs, chip * 2 + 1 - core)]
    barrier = pltpu.get_barrier_semaphore()
    for f, t in links:
        pl.semaphore_signal(
            barrier, inc=1, device_id={"fs": f, "tp": t}, device_id_type=pl.DeviceIdType.MESH
        )

    inner = bit == entry(group)
    outer = jnp.logical_not(inner)

    def remote(src, dst, send_sem, recv_sem, f, t):
        return pltpu.make_async_remote_copy(
            src_ref=src, dst_ref=dst, send_sem=send_sem, recv_sem=recv_sem,
            device_id={"fs": f, "tp": t}, device_id_type=pl.DeviceIdType.MESH,
        )

    small[0].wait()
    gain = jnp.transpose(jnp.broadcast_to(gain_ref[...], (cols, rows)))
    loads[0].wait()
    loads[1].wait()
    loads[2].start()
    loads[3].start()
    experts_all = master.shape[1]
    for e in range(experts_all):
        for kind in (0, 1):
            piece_gu[e // FINE, e % 2, (e % FINE) // 2, kind] = (gain * master[kind, e]).astype(bf16)
    pl.semaphore_wait(barrier, len(links))

    count = 4 * groups
    keys = [(r, bb, jj) for r in range(groups) for bb in (0, 1) for jj in (0, 1)]

    class Route:
        def __init__(self, piece, whole, send_sem, recv_sem):
            self.piece, self.whole, self.lead = piece, whole, (slice(None),) * (len(whole.shape) - 2)
            self.send_sem, self.recv_sem = send_sem, recv_sem

        def region(self, f, t):
            return self.whole.at[self.lead + (block(f), lanes(t))]

        def move(self, src, dst, sent, received, f, t):
            return remote(src, dst, self.send_sem.at[sent], self.recv_sem.at[received], f, t)

        def src(self, key):
            return self.region(source(*key), tp) if any(key) else self.piece.at[group, side]

        def land(self, key):
            r, bb, jj = key
            k = keys.index(key)
            if key == (0, 0, 1):
                piece = self.piece.at[group, flipped(side, 1)]
                return self.move(piece, self.region(fs, tp), k, k, member(group, 0, 1), tp)
            first = key if r else (0, 0, jj)
            here = self.region(source(*first), tp)
            return self.move(self.src(first), here, k, k, member(group, 1, 0), tp)

        def direct(self, r, jj):
            j = flipped(side, jj)
            to = ahead(r) * FINE + entry(ahead(r)) * 2 + j
            slot = r * 4 + flipped(bit, entry(group)) * 2 + jj
            piece = self.piece.at[ahead(r), j]
            return self.move(piece, self.region(fs, tp), count + r * 2 + jj, slot, to, tp)

        def across(self, key, q):
            here = self.region(source(*key), tp)
            k = count + keys.index(key) * (chips - 1) + q - 1
            return self.move(self.src(key), here, k + 2 * groups, k, fs, chip_ahead(q) * 2 + core)

        def beside(self, key, q):
            here = self.region(source(*key), chip_behind(q) * 2 + core)
            src = self.src(key) if q == 0 else here
            k = count * chips + keys.index(key) * chips + q
            return self.move(src, here, k + 2 * groups, k, fs, chip * 2 + 1 - core)

        def hand(self, key):
            for q in range(1, chips):
                self.across(key, q).start()
            self.beside(key, 0).start()

        def arrived(self, key, forward=False):
            self.land(key).wait_recv()
            if forward:
                self.land(key).start()
            if key == (0, 0, 1):
                self.land((0, 1, 1)).start()
            self.hand(key)

        def crossed(self, key):
            for q in range(1, chips):
                self.across(key, q).wait_recv()
                self.beside(key, q).start()

        def directs(self):
            for r in range(1, groups):
                for jj in (0, 1):
                    self.direct(r, jj).start()

        def drain(self):
            for key in keys:
                if any(key) and not key[0]:
                    self.land(key).wait_send()
                for q in range(chips):
                    if q:
                        self.across(key, q).wait_send()
                    self.beside(key, q).wait_send()
            for r in range(1, groups):
                for jj in (0, 1):
                    self.direct(r, jj).wait_send()

            @pl.when(inner)
            def _():
                for key in keys[4:]:
                    self.land(key).wait_send()

    gu = Route(piece_gu, w_gu, gsend, grecv)
    dn = Route(piece_dn, w_dn, dsend, drecv)

    gu.land((0, 0, 1)).start()
    gu.land((0, 1, 0)).start()
    gu.hand((0, 0, 0))
    pl.when(inner)(gu.directs)
    keep_gu = pltpu.make_async_copy(piece_gu.at[group, side], gu.region(fs, tp), lsem.at[4])
    keep_gu.start()

    for copy in small[1:]:
        copy.wait()
    loads[2].wait()
    pad = max(8, groups)
    away = group_ref[...] - group
    away = jnp.where(away < 0, away + groups, away)
    which = lax.broadcasted_iota(jnp.int32, (pad, toks), 0)
    mine = (which == away).astype(f32)
    first = lax.broadcasted_iota(jnp.int32, (toks, toks), 0)
    second = lax.broadcasted_iota(jnp.int32, (toks, toks), 1)
    before = jnp.dot(
        mine.astype(bf16), (first < second).astype(f32).astype(bf16), preferred_element_type=f32
    )
    slot = jnp.sum(mine * (before + (which * cap).astype(f32)), axis=0, keepdims=True)
    placing = (first.astype(f32) == slot).astype(f32)
    place[...] = placing.astype(bf16)
    finer = lax.broadcasted_iota(jnp.int32, (8, toks), 0)
    shares = jnp.zeros((8, toks), f32)
    for k in range(fine_ref.shape[0]):
        shares += jnp.where(finer == fine_ref[k : k + 1, :], weight_ref[k : k + 1, :], 0.0)
    shares = lax.dot_general(
        shares, placing, (((1,), (1,)), ((), ())),
        preferred_element_type=f32, precision=lax.Precision.HIGHEST,
    )

    def normed(r):
        raw = jnp.dot(place[r * cap : (r + 1) * cap, :], tok[...], preferred_element_type=f32)
        scale = lax.rsqrt(jnp.mean(raw * raw, axis=1, keepdims=True) + EPS)
        return (raw * scale).astype(bf16)

    def at(r, jj):
        return pl.ds((r * 2 + jj) * cap, cap)

    share[0, 0] = shares[:, :cap]
    for r in range(1, groups):
        far_share[r - 1] = shares[:, r * cap : (r + 1) * cap]
    x_rows[at(0, 0), :] = normed(0)
    mate = member(group, 0, 1)
    parts = 2
    step = cap // parts

    def rows_move(k, src, dst, f):
        return remote(src, dst, tsend.at[k], trecv.at[k], f, tp)

    def near():
        return [
            rows_move(0, share.at[0, 0], share.at[0, 1], mate),
            rows_move(1, x_rows.at[at(0, 0)], x_rows.at[at(0, 1)], mate),
        ]

    def far(r):
        to, base = member(ahead(r), 0, 0), 2 + (r - 1) * 2 * (parts + 1)
        moves = [rows_move(base, far_share.at[r - 1], share.at[r, 0], to)]
        for p in range(parts):
            here = pl.ds(r * 2 * cap + p * step, step)
            src = far_rows.at[r - 1, pl.ds(p * step, step)]
            moves.append(rows_move(base + 1 + p, src, x_rows.at[here], to))
        return moves

    def passed(r):
        base = 2 + (r - 1) * 2 * (parts + 1) + parts + 1
        moves = [rows_move(base, share.at[r, 0], share.at[r, 1], mate)]
        for p in range(parts):
            here = pl.ds(r * 2 * cap + p * step, step)
            there = pl.ds((r * 2 + 1) * cap + p * step, step)
            moves.append(rows_move(base + 1 + p, x_rows.at[here], x_rows.at[there], mate))
        return moves

    def start_far():
        for r in range(1, groups):
            for move in far(r):
                move.start()

    def pass_far():
        for r in range(1, groups):
            for landed, move in zip(far(r), passed(r)):
                landed.wait_recv()
                move.start()

    for move in near():
        move.start()
    for r in range(1, groups):
        far_rows[r - 1] = normed(r)

    loads[3].wait()
    for e in range(experts_all):
        piece_dn[e // FINE, e % 2, (e % FINE) // 2] = master[2, e].astype(bf16)
    keep_dn = pltpu.make_async_copy(piece_dn.at[group, side], dn.region(fs, tp), lsem.at[5])
    keep_dn.start()
    others = range(1, groups)
    inner_order = [(0, 0, 0), (0, 1, 0), (0, 0, 1)]
    inner_order += [(r, 0, jj) for r in others for jj in (0, 1)] + [(0, 1, 1)]
    inner_order += [(r, 1, jj) for r in others for jj in (0, 1)]
    outer_order = [(0, 0, 0), (0, 0, 1), (0, 1, 0), (0, 1, 1)]
    outer_order += [(r, bb, jj) for r in others for bb in (0, 1) for jj in (0, 1)]
    ahead_of = 3

    def route_gates(order, forward):
        done = 0
        for k, key in enumerate(order[1:]):
            gu.arrived(key, forward and key[0] > 0)
            if key == (0, 0, 1):
                dn.land((0, 0, 1)).start()
                dn.beside((0, 0, 0), 0).start()
                if not forward:
                    gu.directs()
                    start_far()
            if k >= ahead_of:
                gu.crossed(order[done])
                done += 1
        if forward:
            start_far()
        for q in range(1, chips):
            dn.across((0, 0, 0), q).start()

    pl.when(inner)(lambda: route_gates(inner_order, True))
    pl.when(outer)(lambda: route_gates(outer_order, False))

    def apply_rows(start, count, s, lane0, lane_count):
        here = pl.ds(start * cap, count * cap)
        x = x_rows[here, :]
        at_lanes = pl.ds(pl.multiple_of(lane0, cols), lane_count)
        gate_value = jnp.dot(x, w_gu[s, 0, :, at_lanes], preferred_element_type=f32)
        upward = jnp.dot(x, w_gu[s, 1, :, at_lanes], preferred_element_type=f32)
        fine = s * 2 + side
        chosen = []
        for i in range(start, start + count):
            flat = jnp.transpose(share[i // 2, i % 2])
            lane = lax.broadcasted_iota(jnp.int32, flat.shape, 1)
            chosen.append(jnp.sum(jnp.where(lane == fine, flat, 0.0), axis=1, keepdims=True))
        weight = jnp.concatenate(chosen, axis=0)
        value = gate_value / (1.0 + jnp.exp(-gate_value)) * upward * weight
        act[here, pl.ds(pl.multiple_of(s * hidden + lane0, cols), lane_count)] = value.astype(bf16)

    keep_gu.wait()
    for key in keys:
        if any(key):
            gu.beside(key, 0).wait_recv()
    gu.beside((0, 0, 0), 0).wait_recv()
    for move in near():
        move.wait_recv()
    pair = 2 * cols
    for s in (0, 1):
        apply_rows(0, 2, s, chip * pair, pair)

    def finish_gates(order, forward):
        rest = order[len(order) - 1 - ahead_of :]
        dn.land((0, 0, 1)).wait_recv()
        dn.hand((0, 0, 1))
        if not forward:
            dn.land((0, 1, 0)).start()
            dn.land((0, 1, 1)).start()
        for k, key in enumerate(rest):
            if k == len(rest) - (2 if forward else 2):
                pass_far()
            if k == len(rest) - (0 if forward else 1):
                if forward:
                    dn.land((0, 1, 0)).start()
                    dn.land((0, 1, 1)).start()
                dn.directs()
            gu.crossed(key)
        if forward:
            dn.land((0, 1, 0)).start()
            dn.land((0, 1, 1)).start()
            dn.directs()

    pl.when(inner)(lambda: finish_gates(inner_order, True))
    pl.when(outer)(lambda: finish_gates(outer_order, False))
    for key in keys:
        for q in range(1, chips):
            gu.beside(key, q).wait_recv()
    for q in range(1, chips):
        for s in (0, 1):
            apply_rows(0, 2, s, chip_behind(q) * pair, pair)
    outs = [
        pltpu.make_async_copy(w_gu.at[bit, 0], gate_out.at[0], lsem.at[6]),
        pltpu.make_async_copy(w_gu.at[bit, 1], up_out.at[0], lsem.at[7]),
    ]
    for copy in outs:
        copy.start()

    keep_dn.wait()
    span = 2 * rows
    steps = [(0, 0), (0, 1)] + [(r, bb) for r in range(1, groups) for bb in (1, 0)]

    def columns(n, cut, cuts, base=group):
        r, bb = steps[n]
        wide = span // cuts
        grp = (base + groups - r) % groups
        pick = flipped(entry(grp) if r else bit, bb)
        start = (grp * FINE + pick * 2) * rows + cut * wide
        return pl.ds(pl.multiple_of(start, wide), wide)

    crossing, home = {}, {}

    def ready(n):
        r, bb = steps[n]
        for jj in (0, 1):
            for q in range(chips):
                dn.beside((r, bb, jj), q).wait_recv()

    def produce(n, r, cut, cuts):
        here = columns(n, cut, cuts)
        mine = pl.ds(r * 2 * cap, 2 * cap)
        out = jnp.zeros((2 * cap, span // cuts), f32)
        for s in (0, 1):
            out += lax.dot_general(
                act[mine, s * hidden : (s + 1) * hidden], w_dn[s, here, :],
                (((1,), (1,)), ((), ())), preferred_element_type=f32,
            )
        y_send[r, :, here] = out[cap:].astype(bf16)
        part[r, :, here] = out[:cap]
        k = len(crossing)
        crossing[n, r, cut, cuts] = remote(
            y_send.at[r, :, here], y_recv.at[r, :, here], ysend.at[k], yrecv.at[k], mate, tp
        )
        crossing[n, r, cut, cuts].start()
        waiting.append((n, r, cut, cuts))

    def combine(n, r, cut, cuts):
        here = columns(n, cut, cuts)
        crossing[n, r, cut, cuts].wait_recv()
        total = (part[r, :, here] + y_recv[r, :, here].astype(f32)).astype(bf16)
        if r == 0:
            ret[0, :, here] = total
        else:
            z_send[r - 1, :, here] = total
            k = len(home)
            home[n, r, cut] = remote(
                z_send.at[r - 1, :, here], ret.at[r, :, here], zsend.at[k], zrecv.at[k],
                member(behind(r), 0, 0), tp,
            )
            home[n, r, cut].start()

    waiting = []
    last = len(steps) - 1

    def cuts_of(n):
        return 2 if n in (last,) else 1


    def far_down(bb):
        for r in others:
            for jj in (0, 1):
                dn.arrived((r, bb, jj), True)

    def far_down_outer(bb):
        for r in others:
            for jj in (0, 1):
                dn.arrived((r, bb, jj))

    def near_down():
        dn.arrived((0, 1, 0))
        dn.arrived((0, 1, 1))

    pl.when(outer)(near_down)
    for r in others:
        for move in passed(r):
            move.wait_recv()
        for s in (0, 1):
            for half in range(chips):
                apply_rows(2 * r, 2, s, half * pair, pair)
    pl.when(inner)(near_down)
    for jj in (0, 1):
        dn.crossed((0, 0, jj))
    pl.when(inner)(lambda: far_down(1))
    ready(0)
    for r in reversed(range(groups)):
        for cut in range(cuts_of(0)):
            produce(0, r, cut, cuts_of(0))
    pl.when(outer)(lambda: far_down_outer(1))
    pl.when(inner)(lambda: far_down(0))
    def settle(far_only):
        for item in [w for w in waiting if w[1] or not far_only]:
            waiting.remove(item)
            combine(*item)

    for n in range(1, len(steps)):
        for jj in (0, 1):
            dn.crossed((*steps[n], jj))
        settle(True)
        if n == 2:
            pl.when(outer)(lambda: far_down_outer(0))
        ready(n)
        for r in reversed(range(groups)):
            for cut in range(cuts_of(n)):
                produce(n, r, cut, cuts_of(n))
            if r == 1:
                for item in [w for w in waiting if w[0] < n]:
                    waiting.remove(item)
                    combine(*item)
    outs.append(pltpu.make_async_copy(w_dn.at[bit], down_out.at[0], lsem.at[8]))
    outs[-1].start()
    outs.append(pltpu.make_async_copy(place, place_out, lsem.at[10]))
    outs[-1].start()
    settle(True)
    settle(False)
    outs.append(pltpu.make_async_copy(ret.at[0], ret_out.at[0], lsem.at[9]))
    outs[-1].start()
    gu.drain()
    dn.drain()
    for move in near():
        move.wait_send()
    for r in others:
        for move in far(r) + passed(r):
            move.wait_send()
    for k, ((n, r, cut), copy) in enumerate(home.items()):
        copy.wait_recv()
        here = columns(n, cut, cuts_of(n), ahead(r))
        outs.append(
            pltpu.make_async_copy(ret.at[r, :, here], ret_out.at[r, :, here], lsem.at[11 + k])
        )
        outs[-1].start()
    for copy in list(crossing.values()) + list(home.values()):
        copy.wait_send()
    for copy in outs:
        copy.wait()


def publish_kernel(
    place_ref, ret_ref, gate_ref, up_ref, down_ref, mixed_out, gate_out, up_out, down_out,
    mixed, out_sem, row_sem,
):
    writes = [
        pltpu.make_async_copy(src, dst, out_sem.at[k])
        for k, (src, dst) in enumerate(
            ((gate_ref, gate_out), (up_ref, up_out), (down_ref, down_out))
        )
    ]
    for write in writes:
        write.start()
    width = ret_ref.shape[1]
    chunk = min(width, 512)
    for c in range(0, width, chunk):
        here = pl.ds(c, chunk)
        mixed[:, here] = lax.dot_general(
            place_ref[...], ret_ref[:, here], (((0,), (0,)), ((), ())),
            preferred_element_type=jnp.float32,
        ).astype(jnp.bfloat16)
    last = pltpu.make_async_copy(mixed, mixed_out, row_sem)
    last.start()
    last.wait()
    for write in writes:
        write.wait()


def publish(placed, returned, gate, up, down):
    toks, width = returned.shape
    anywhere = pl.BlockSpec(memory_space=pl.ANY)
    local_spec = pl.BlockSpec(memory_space=pltpu.VMEM)
    whole = jax.ShapeDtypeStruct(gate.shape, gate.dtype)
    return pl.pallas_call(
        publish_kernel,
        out_shape=(jax.ShapeDtypeStruct((toks, width), returned.dtype), whole, whole, whole),
        in_specs=[local_spec] * 2 + [anywhere] * 3,
        out_specs=(anywhere,) * 4,
        scratch_shapes=[
            pltpu.VMEM((toks, width), returned.dtype),
            pltpu.SemaphoreType.DMA((3,)),
            pltpu.SemaphoreType.DMA,
        ],
        compiler_params=pltpu.CompilerParams(vmem_limit_bytes=12 << 20),
        cost_estimate=pl.CostEstimate(
            flops=2 * toks * toks * width, bytes_accessed=6 * gate.size * 2, transcendentals=0
        ),
    )(placed, returned, gate, up, down)


def fused(
    tokens, expert_group, expert_fine, route_weight, norm_gain, gate_master, up_master, down_master
):
    toks, width = tokens.shape
    fs_size, tp_size = lax.axis_size("fs"), lax.axis_size("tp")
    experts_all, rows, cols = gate_master.shape
    groups, chips, hidden = experts_all // FINE, tp_size // 2, cols * tp_size
    cap = toks // groups
    bf16, f32 = jnp.bfloat16, jnp.float32
    sources = groups * 4
    sends = sources * 2 * chips + 2 * groups
    moves = 2 + (groups - 1) * 6
    steps = 2 * groups
    vmem, dma = pltpu.VMEM, pltpu.SemaphoreType.DMA
    anywhere = pl.BlockSpec(memory_space=pl.ANY)
    sent = 2 * (3 * width * hidden * 2 + 6 * toks * width)
    placed, returned, *ready = pl.pallas_call(
        functools.partial(fused_kernel, groups, chips, cap),
        out_shape=(
            vmem((toks, toks), bf16),
            vmem((groups, cap, width), bf16),
            vmem((1, width, hidden), bf16),
            vmem((1, width, hidden), bf16),
            vmem((1, width, hidden), bf16),
        ),
        in_specs=[pl.BlockSpec(memory_space=pltpu.HBM)] * 8,
        out_specs=(anywhere,) * 5,
        scratch_shapes=[
            vmem((3, experts_all, rows, cols), f32),
            vmem((toks, width), bf16),
            vmem((groups, 2, 2, 2, rows, cols), bf16),
            vmem((groups, 2, 2, rows, cols), bf16),
            vmem((2, 2, width, hidden), bf16),
            vmem((2, width, hidden), bf16),
            vmem((2 * groups * cap, width), bf16),
            vmem((groups - 1, cap, width), bf16),
            vmem((groups, 2, 8, cap), f32),
            vmem((groups - 1, 8, cap), f32),
            vmem((2 * groups * cap, 2 * hidden), bf16),
            vmem((groups, cap, width), bf16),
            vmem((groups, cap, width), bf16),
            vmem((groups, cap, width), f32),
            vmem((groups - 1, cap, width), bf16),
            vmem((groups, cap, width), bf16),
            vmem((toks, toks), bf16),
            vmem((1, rows), f32),
            vmem((1, toks), jnp.int32),
            vmem((expert_fine.shape[1], toks), jnp.int32),
            vmem((route_weight.shape[1], toks), f32),
            dma((4,)),
            dma((11 + (steps + 2) * (groups - 1),)),
            dma((sends,)), dma((sends,)), dma((sends,)), dma((sends,)),
            dma((moves,)), dma((moves,)),
            dma(((steps + 2) * groups,)), dma(((steps + 2) * groups,)),
            dma(((steps + 2) * (groups - 1),)), dma(((steps + 2) * (groups - 1),)),
        ],
        compiler_params=pltpu.CompilerParams(
            collective_id=1, has_side_effects=True, vmem_limit_bytes=56 << 20
        ),
        cost_estimate=pl.CostEstimate(
            flops=12 * groups * cap * 2 * width * hidden, bytes_accessed=sent, transcendentals=0
        ),
    )(
        norm_gain[None, :], expert_group[None, :], expert_fine.T, route_weight.T,
        tokens, gate_master, up_master, down_master,
    )
    return publish(placed, returned.reshape(toks, width), *ready)


def step(*args):
    tp_size = lax.axis_size("tp")
    gate_master = args[5]
    groups = gate_master.shape[0] // FINE
    if lax.axis_size("fs") == gate_master.shape[0] and tp_size > 2 and groups > 1 and gate_master.shape[2] % 128 == 0:
        return fused(*args)
    return local(*args)


def solution(mesh):
    in_specs = (
        P(("fs", "tp"), None),
        P(("fs", "tp")),
        P(("fs", "tp"), None),
        P(("fs", "tp"), None),
        P("fs"),
        P(None, "fs", "tp"),
        P(None, "fs", "tp"),
        P(None, "fs", "tp"),
    )
    out_specs = (
        P(("fs", "tp"), None),
        P("fs", None, None),
        P("fs", None, None),
        P("fs", None, None),
    )
    return jax.shard_map(step, mesh=mesh, in_specs=in_specs, out_specs=out_specs, check_vma=False)
```
